768 devices in a mesh: rep: 3 (over z_hi), fs: 32 (over z_lo, y), tp: 8 (over x, core).
Axes of the slice: x: 4, y: 8, z: 12 (z_hi: 3, z_lo: 4; z = z_hi * 4 + z_lo), core: 2. Of those that a mesh axis runs over, the one named last changes fastest.
Arguments:
- tokens: bfloat16 [49152, 2048], P(('rep', 'fs')), may hold values from -6 to 6
- norm_gain: float32 [2048], replicated, may hold values from 0.1 to 1.9
- gate_weight: bfloat16 [2048, 5632], P('fs', 'tp'), may hold values from -0.125 to 0.125
- up_weight: bfloat16 [2048, 5632], P('fs', 'tp'), may hold values from -0.125 to 0.125
- down_weight: bfloat16 [5632, 2048], P('tp', 'fs'), may hold values from -0.078125 to 0.078125
Outputs:
- branch_out: bfloat16 [49152, 2048], P(('rep', 'fs'))
The draws below stay inside these ranges and needn't reach their ends.
All inputs are finite; a program needn't handle non-finite values.
Results may differ from the reference program's by a relative error of at most 0.014.
Values may be sent and summed in bfloat16 or wider, within the bound.
No kernel may reach another device: no remote copies, remote signals or barrier semaphores. Data moves between devices by JAX's collectives and lax.ppermute only.
A program may use at most 32 MiB of HBM per device.

```python
import jax
import jax.numpy as jnp
from jax import lax

D = 2048
FF = 5632
TOKENS = 49152
N_TP = 8


def steps_of(key, shape, cuts, low, top_value):
    def one(axis_at, blocks):
        steps = jax.random.uniform(jax.random.fold_in(jax.random.fold_in(key, 6), axis_at), (blocks,), jnp.float32, low / len(cuts), top_value / len(cuts))
        return jnp.repeat(jnp.exp(steps), shape[axis_at] // blocks).reshape((-1,) + (1,) * (len(shape) - axis_at - 1))

    level = one(*cuts[0])
    for cut in cuts[1:]:
        level = level * one(*cut)
    return level


def gaussian(rng, shape, scale, most, split=(), kind=jnp.bfloat16):
    drawn = scale * jax.random.normal(rng, shape, jnp.float32)
    if split:
        drawn = drawn * steps_of(rng, shape, split, -0.22, 0.18)
    return jnp.clip(drawn, -most, most).astype(kind)


def setup_inputs(seed: int = 0) -> dict:
    streams_of = jax.random.split(jax.random.key(seed), 6)
    return {
        "tokens": gaussian(streams_of[0], (TOKENS, D), 1.0, 6.0, ((0, 96),)),
        "norm_gain": jnp.clip(1.0 + 0.18 * jax.random.normal(streams_of[1], (D,), jnp.float32), 0.1, 1.9),
        "gate_weight": gaussian(streams_of[2], (D, FF), D ** -0.5, 0.125, ((0, 32), (1, 8))),
        "up_weight": gaussian(streams_of[3], (D, FF), D ** -0.5, 0.125, ((0, 32), (1, 8))),
        "down_weight": gaussian(streams_of[4], (FF, D), FF ** -0.5, 0.078125, ((0, 8), (1, 32))),
    }


def reference(tokens, norm_gain, gate_weight, up_weight, down_weight):
    wide_tok = tokens.astype(jnp.float32)
    scale = jax.lax.rsqrt(lax.optimization_barrier(jnp.mean(wide_tok * wide_tok, axis=-1, keepdims=True)) + 1e-06)
    normed = (wide_tok * scale * norm_gain).astype(jnp.bfloat16)
    gate = jnp.dot(normed, gate_weight, preferred_element_type=jnp.float32)
    up = jnp.dot(normed, up_weight, preferred_element_type=jnp.float32)
    hidden = (jax.nn.silu(gate) * up).astype(jnp.bfloat16)
    width = FF // N_TP
    total = jnp.zeros((hidden.shape[0], D), jnp.float32)
    for block in range(N_TP):
        partial_value = jnp.dot(hidden[:, block * width:(block + 1) * width], down_weight[block * width:(block + 1) * width], preferred_element_type=jnp.float32).astype(jnp.bfloat16)
        total = total + partial_value.astype(jnp.float32)
    return total.astype(jnp.bfloat16)
```

```python
import functools

import jax
import jax.numpy as jnp
from jax import lax
from jax.experimental import pallas as pl
from jax.experimental.pallas import tpu as pltpu
from jax.sharding import Mesh
from jax.sharding import PartitionSpec as P


Z = ("zh", "zl")
NZ, NY, ROWS, HID, GU = 4, 8, 64, 704, 1408
D = 2048


def ring(n, step):
    return [(i, (i + step) % n) for i in range(n)]


def z_from(x, step):
    return lax.ppermute(x, Z, ring(12, -step))


def y_from(x, step):
    return lax.ppermute(x, "y", ring(NY, -step))


def other_core(x):
    return lax.ppermute(x, "c", ring(2, 1))


def lanes_paired(a, b):
    parts = []
    for j in range(5):
        parts += [a[:, 128 * j : 128 * j + 128], b[:, 128 * j : 128 * j + 128]]
    parts += [a[:, 640:], b[:, 640:]]
    return jnp.concatenate(parts, axis=1)


def packed(gate, up, down):
    down_t = down.T
    return jnp.concatenate([lanes_paired(gate, up), lanes_paired(down_t[:32], down_t[32:])], axis=0)


def gathered(own):
    n = own.shape[0]
    above = z_from(own, 1)
    pair = jnp.concatenate([own, above], axis=0)
    got = [(pair, [(0, 0), (1, 0)])]
    lo, hi = y_from(pair, -1), y_from(pair, 1)
    got += [(z_from(own, -1), [(-1, 0)]), (z_from(above, 1), [(2, 0)])]
    for k in (1, 2, 3):
        got += [(lo, [(0, -k), (1, -k)]), (hi, [(0, k), (1, k)])]
        here = jnp.concatenate([lo[:n], hi[:n]], axis=0)
        there = jnp.concatenate([lo[n:], hi[n:]], axis=0)
        if k < 3:
            lo, hi = y_from(lo, -1), y_from(hi, 1)
        else:
            lo, hi = y_from(lo[:n], -1), y_from(hi[n:], 1)
        got += [(z_from(here, -1), [(-1, -k), (-1, k)]), (z_from(there, 1), [(2, -k), (2, k)])]
    got += [(lo, [(0, 4)]), (hi, [(1, 4)])]
    got += [(z_from(lo, -1), [(-1, 4)]), (z_from(hi, 1), [(2, 4)])]
    return got


def ffn_kernel(places, at_ref, normed_ref, *refs):
    blocks = refs[: len(places)]
    theirs_ref, mine_ref, gu_ref, down_ref, hid_ref = refs[len(places) :]
    z, y, core = at_ref[0], at_ref[1], at_ref[2]
    for block, where in zip(blocks, places):
        for k, (dz, dy) in enumerate(where):
            row = (lax.rem(z + (dz + NZ), NZ) * NY + lax.rem(y + (dy + NY), NY)) * ROWS
            row = pl.multiple_of(row, ROWS)
            at = 96 * k
            gu_ref[pl.ds(row, ROWS), :] = block[at : at + 64, :]
            for j in range(5):
                lanes = slice(128 * j, 128 * j + 128)
                down_ref[pl.ds(row, 32), lanes] = block[at + 64 : at + 96, 256 * j : 256 * j + 128]
                down_ref[pl.ds(row + 32, 32), lanes] = block[at + 64 : at + 96, 256 * j + 128 : 256 * j + 256]
            down_ref[pl.ds(row, 32), 640:704] = block[at + 64 : at + 96, 1280:1344]
            down_ref[pl.ds(row + 32, 32), 640:704] = block[at + 64 : at + 96, 1344:1408]

    def gated(pre, width):
        gate, up = pre[:, :width], pre[:, width:]
        return (gate / (1.0 + jnp.exp(-gate)) * up).astype(jnp.bfloat16)

    for j in range(5):
        pre = jnp.dot(normed_ref[...], gu_ref[:, 256 * j : 256 * j + 256], preferred_element_type=jnp.float32)
        hid_ref[:, :, 128 * j : 128 * j + 128] = gated(pre, 128).reshape(2, 256, 128)
    pre = jnp.dot(normed_ref[...], gu_ref[:, 1280:1408], preferred_element_type=jnp.float32)
    hid_ref[:, :, 640:704] = gated(pre, 64).reshape(2, 256, 64)

    for half, out_ref in ((1 - core, theirs_ref), (core, mine_ref)):
        hid = hid_ref[half]
        for j in range(8):
            rows = slice(256 * j, 256 * j + 256)
            out_ref[:, rows] = lax.dot_general(
                hid, down_ref[rows, :], (((1,), (1,)), ((), ())), preferred_element_type=jnp.float32
            ).astype(jnp.bfloat16)


def ffn(at, normed, got):
    arrays = [a for a, _ in got]
    places = [w for _, w in got]
    vmem = pl.BlockSpec(memory_space=pltpu.VMEM)
    half = jax.ShapeDtypeStruct((256, D), jnp.bfloat16)
    return pl.pallas_call(
        functools.partial(ffn_kernel, places),
        out_shape=(half, half),
        in_specs=[pl.BlockSpec(memory_space=pltpu.SMEM)] + [vmem] * (1 + len(arrays)),
        out_specs=(vmem, vmem),
        scratch_shapes=[
            pltpu.VMEM((D, GU), jnp.bfloat16),
            pltpu.VMEM((D, HID), jnp.bfloat16),
            pltpu.VMEM((2, 256, HID), jnp.bfloat16),
        ],
        compiler_params=pltpu.CompilerParams(vmem_limit_bytes=40 * 2**20),
        cost_estimate=pl.CostEstimate(flops=4_430_000_000, bytes_accessed=13_000_000, transcendentals=360_448),
        name="ffn",
    )(at, normed, *arrays)


def per_device(tokens, norm_gain, gate_weight, up_weight, down_weight):
    core = lax.axis_index("c")
    at = jnp.stack([lax.axis_index("zl"), lax.axis_index("y"), core]).astype(jnp.int32)
    got = gathered(packed(gate_weight, up_weight, down_weight))
    wide_tok = tokens.astype(jnp.float32)
    scale = lax.rsqrt(jnp.mean(wide_tok * wide_tok, axis=-1, keepdims=True) + 1e-06)
    normed = (wide_tok * scale * norm_gain).astype(jnp.bfloat16)
    theirs, mine = ffn(at, normed, got)
    summed = mine.astype(jnp.float32) + other_core(theirs).astype(jnp.float32)
    parts = lax.all_to_all(summed.astype(jnp.bfloat16).reshape(4, 64, D), "x", 0, 0, tiled=True)
    rows = jnp.sum(parts.astype(jnp.float32), axis=0).astype(jnp.bfloat16)
    near = lax.all_to_all(jnp.broadcast_to(rows[None], (4, 64, D)), "x", 0, 0, tiled=True).reshape(256, D)
    far = other_core(near)
    first, second = jnp.where(core == 0, near, far), jnp.where(core == 0, far, near)
    return jnp.concatenate([first, second], axis=0)


def solution(mesh):
    split = Mesh(mesh.devices.reshape(mesh.shape["rep"], 4, 8, 4, 2), ("zh", "zl", "y", "x", "c"))
    tok = P(("zh", "zl", "y"), None)
    fs, tp = ("zl", "y"), ("x", "c")
    placed = (tok, P(), P(fs, tp), P(fs, tp), P(tp, fs))
    return jax.shard_map(per_device, mesh=split, in_specs=placed, out_specs=tok, check_vma=False)
```

```python
import functools

import jax
import jax.numpy as jnp
from jax import lax
from jax.experimental import pallas as pl
from jax.experimental.pallas import tpu as pltpu
from jax.sharding import Mesh
from jax.sharding import PartitionSpec as P


NZ, NY, HID, GU = 4, 8, 704, 1408
D = 2048
HALF = 48
VMEM = pl.BlockSpec(memory_space=pltpu.VMEM)
SMEM = pl.BlockSpec(memory_space=pltpu.SMEM)
ANY = pl.BlockSpec(memory_space=pl.ANY)
RINGS = {"z": (("zh", "zl", "c"), 12), "y": (("y", "c"), 8), "x": (("x", "c"), 4)}


def hop(x, ring, step):
    axes, n = RINGS[ring]
    pairs = [(2 * ((i + (1 - 2 * c) * step) % n) + c, 2 * i + c) for i in range(n) for c in range(2)]
    return lax.ppermute(x, axes, pairs)


def other_core(x):
    return lax.ppermute(x, "c", [(0, 1), (1, 0)])


def pack_kernel(gate_hbm, up_hbm, down_hbm, out_ref, gate_ref, up_ref, down_ref, sems):
    pairs = ((gate_hbm, gate_ref), (up_hbm, up_ref), (down_hbm, down_ref))
    copies = [pltpu.make_async_copy(source, to, sems.at[k]) for k, (source, to) in enumerate(pairs)]
    for copy in copies:
        copy.start()
    for copy in copies:
        copy.wait()

    def pair(at, rows, a_ref, a_at, b_ref, b_at):
        for j in range(5):
            lanes = slice(128 * j, 128 * j + 128)
            out_ref[at : at + rows, 256 * j : 256 * j + 128] = a_ref[a_at : a_at + rows, lanes]
            out_ref[at : at + rows, 256 * j + 128 : 256 * j + 256] = b_ref[b_at : b_at + rows, lanes]
        last = [a_ref[a_at : a_at + rows, 640:704], b_ref[b_at : b_at + rows, 640:704]]
        out_ref[at : at + rows, 1280:1408] = jnp.concatenate(last, axis=1)

    for h in range(2):
        pair(HALF * h, 32, gate_ref, 32 * h, up_ref, 32 * h)
        pair(HALF * h + 32, 16, down_ref, 32 * h, down_ref, 32 * h + 16)


def packed(gate, up, down):
    return pl.pallas_call(
        pack_kernel,
        out_shape=jax.ShapeDtypeStruct((2 * HALF, GU), jnp.bfloat16),
        in_specs=[ANY] * 3,
        out_specs=VMEM,
        scratch_shapes=[pltpu.VMEM((64, HID), jnp.bfloat16)] * 3 + [pltpu.SemaphoreType.DMA((3,))],
        compiler_params=pltpu.CompilerParams(vmem_limit_bytes=63 * 2**20),
        name="pack",
    )(gate, up, down.T)


def norm_kernel(tok_ref, gain_ref, out_ref):
    for r in range(0, 512, 64):
        tok = tok_ref[r : r + 64, :].astype(jnp.float32)
        scale = lax.rsqrt(jnp.mean(tok * tok, axis=-1, keepdims=True) + 1e-06)
        normed = tok * scale * gain_ref[...]
        for s in range(16):
            slab = normed[:, 128 * s : 128 * s + 128]
            out_ref[0, s, r : r + 64, :] = slab.astype(jnp.bfloat16)
            out_ref[1, s, r : r + 64, :] = pltpu.roll(slab, 64, 1).astype(jnp.bfloat16)


def normalized(tokens, gain):
    return pl.pallas_call(
        norm_kernel,
        out_shape=jax.ShapeDtypeStruct((2, 16, 512, 128), jnp.bfloat16),
        in_specs=[VMEM] * 2,
        out_specs=VMEM,
        compiler_params=pltpu.CompilerParams(vmem_limit_bytes=8 * 2**20),
        cost_estimate=pl.CostEstimate(flops=400_000_000, bytes_accessed=6_000_000, transcendentals=512),
        name="norm",
    )(tokens, gain.reshape(1, D))


def gathered(own):
    top, low = own[:HALF], own[HALF:]
    pair = jnp.concatenate([top, hop(top, "z", -2), low, hop(low, "z", 2)], axis=0)

    def whole(dz, dy):
        return [(dz, dy, 0), (dz + 2, dy, 0), (dz, dy, 1), (dz + 2, dy, 1)]

    early, late = [(pair, whole(0, 0))], []
    lo, hi = hop(pair, "y", -1), hop(pair, "y", 1)
    early.append((hop(pair, "z", -1), whole(-1, 0)))
    for k in (1, 2, 3):
        early += [(lo, whole(0, -k)), (hi, whole(0, k))]
        up, down = hop(lo, "z", -1), hop(hi, "z", 1)
        (early if k < 3 else late).extend([(up, whole(-1, -k)), (down, whole(1, k))])
        lo = hop(lo, "y", -1)
        if k < 3:
            hi = hop(hi, "y", 1)
    late += [(lo, whole(0, -4)), (hop(lo, "z", -1), whole(-1, -4))]
    return early, late


def shard_index(at_ref, dz, dy):
    z, y, sign = at_ref[0], at_ref[1], 1 - 2 * at_ref[2]
    return lax.rem(z + sign * dz + 2 * NZ, NZ) * NY + lax.rem(y + sign * dy + 2 * NY, NY)


def place(blocks, places, at_ref, normed_ref, lhs_ref, gu_ref, down_ref):
    low = lax.broadcasted_iota(jnp.int32, (512, 128), 1) < 64
    order = {}
    for block, where in zip(blocks, places):
        for k, (dz, dy, h) in enumerate(where):
            shard = order.setdefault((dz % NZ, dy % NY), len(order))
            index = shard_index(at_ref, dz % NZ, dy % NY)
            at = HALF * k
            gu_ref[64 * shard + 32 * h : 64 * shard + 32 * h + 32, :] = block[at : at + 32, :]
            for part in range(2):
                rows = pl.ds(pl.multiple_of(index * 64 + 32 * h + 16 * part, 16), 16)
                for j in range(5):
                    source = slice(256 * j + 128 * part, 256 * j + 128 * part + 128)
                    down_ref[rows, 128 * j : 128 * j + 128] = block[at + 32 : at + 48, source]
                down_ref[rows, 640:704] = block[at + 32 : at + 48, 1280 + 64 * part : 1344 + 64 * part]
    shards = list(order)
    for j in range(0, len(shards), 2):
        halves = []
        for side in range(2):
            dz, dy = shards[j + side]
            index = shard_index(at_ref, dz, dy)
            odd = lax.rem(index, 2)
            halves.append(normed_ref[odd if side == 0 else 1 - odd, lax.div(index, 2)])
        lhs_ref[:, 64 * j : 64 * j + 128] = jnp.where(low, halves[0], halves[1])


def first_kernel(places, at_ref, normed_ref, *refs):
    blocks = refs[: len(places)]
    pre_ref, down_ref, lhs_ref, gu_ref = refs[len(places) :]
    place(blocks, places, at_ref, normed_ref, lhs_ref, gu_ref, down_ref)
    for j in range(0, GU, 256):
        lanes = slice(j, min(j + 256, GU))
        pre_ref[:, lanes] = jnp.dot(lhs_ref[...], gu_ref[:, lanes], preferred_element_type=jnp.float32)


def last_kernel(places, at_ref, normed_ref, pre_ref, down_in_ref, *refs):
    blocks = refs[: len(places)]
    theirs_ref, mine_ref, down_ref, lhs_ref, gu_ref, hid_ref = refs[len(places) :]
    place(blocks, places, at_ref, normed_ref, lhs_ref, gu_ref, down_ref)
    core, x = at_ref[2], at_ref[3]

    def gated(j, width):
        lanes = slice(256 * j, 256 * j + 2 * width)
        pre = pre_ref[:, lanes] + jnp.dot(lhs_ref[...], gu_ref[:, lanes], preferred_element_type=jnp.float32)
        gate, up = pre[:, :width], pre[:, width:]
        hid = (gate / (1.0 + jnp.exp(-gate)) * up).astype(jnp.bfloat16)
        hid_ref[:, :, 128 * j : 128 * j + width] = hid.reshape(2, 256, width)

    for j in range(5):
        gated(j, 128)
    gated(5, 64)
    for half, out_ref in ((1 - core, theirs_ref), (core, mine_ref)):
        chunks = [lax.rem(x + (1 - 2 * half) * j + 4, 4) for j in range(4)]
        hid = jnp.concatenate([hid_ref[half, pl.ds(pl.multiple_of(64 * c, 64), 64), :] for c in chunks], axis=0)
        for j in range(8):
            rows = slice(256 * j, 256 * j + 256)
            out_ref[:, rows] = lax.dot_general(
                hid, down_ref[rows, :], (((1,), (1,)), ((), ())), preferred_element_type=jnp.float32
            ).astype(jnp.bfloat16)


def shards_of(items):
    return sum(len(where) for _, where in items) // 2


def ffn(at, normed, early, late):
    down_shape = jax.ShapeDtypeStruct((D, HID), jnp.bfloat16)
    k = 64 * shards_of(early)
    pre, down = pl.pallas_call(
        functools.partial(first_kernel, [w for _, w in early]),
        out_shape=(jax.ShapeDtypeStruct((512, GU), jnp.float32), down_shape),
        in_specs=[SMEM] + [VMEM] * (1 + len(early)),
        out_specs=(VMEM, VMEM),
        scratch_shapes=[pltpu.VMEM((512, k), jnp.bfloat16), pltpu.VMEM((k, GU), jnp.bfloat16)],
        compiler_params=pltpu.CompilerParams(vmem_limit_bytes=24 * 2**20),
        cost_estimate=pl.CostEstimate(flops=2 * 512 * k * GU, bytes_accessed=13_000_000, transcendentals=0),
        name="ffn_first",
    )(at, normed, *[a for a, _ in early])
    k = 64 * shards_of(late)
    half = jax.ShapeDtypeStruct((256, D), jnp.bfloat16)
    return pl.pallas_call(
        functools.partial(last_kernel, [w for _, w in late]),
        out_shape=(half, half, down_shape),
        in_specs=[SMEM] + [VMEM] * (3 + len(late)),
        out_specs=(VMEM,) * 3,
        input_output_aliases={3: 2},
        scratch_shapes=[
            pltpu.VMEM((512, k), jnp.bfloat16),
            pltpu.VMEM((k, GU), jnp.bfloat16),
            pltpu.VMEM((2, 256, HID), jnp.bfloat16),
        ],
        compiler_params=pltpu.CompilerParams(vmem_limit_bytes=24 * 2**20),
        cost_estimate=pl.CostEstimate(flops=2_200_000_000, bytes_accessed=10_000_000, transcendentals=360_448),
        name="ffn_last",
    )(at, normed, pre, down, *[a for a, _ in late])[:2]


def assemble_kernel(at_ref, *refs):
    blocks, out_hbm, sems = refs[:-2], refs[-2], refs[-1]
    core, x = at_ref[2], at_ref[3]
    copies = []
    for k, (block, rows) in enumerate(zip(blocks, (64, 64, 64, 64, 192, 64))):
        half = core if k < 4 else 1 - core
        sign = 1 - 2 * half
        steps = ((0,), (-1,), (1,), (2,), (0, -1, 1), (2,))[k]
        for j, step in enumerate(steps):
            row = 256 * half + 64 * lax.rem(x + sign * step + 4, 4)
            to = out_hbm.at[pl.ds(pl.multiple_of(row, 64), 64), :]
            copies.append(pltpu.make_async_copy(block.at[pl.ds(64 * j, 64), :], to, sems.at[len(copies)]))
    for copy in copies:
        copy.start()
    for copy in copies:
        copy.wait()


def assembled(at, blocks):
    return pl.pallas_call(
        assemble_kernel,
        out_shape=jax.ShapeDtypeStruct((512, D), jnp.bfloat16),
        in_specs=[SMEM] + [VMEM] * len(blocks),
        out_specs=ANY,
        scratch_shapes=[pltpu.SemaphoreType.DMA((8,))],
        compiler_params=pltpu.CompilerParams(vmem_limit_bytes=6 * 2**20),
        name="assemble",
    )(at, *blocks)


def summed_over_x(mine, theirs):
    total = mine.astype(jnp.float32) + other_core(theirs).astype(jnp.float32)
    chunk = [total[64 * j : 64 * j + 64] for j in range(4)]
    passed = hop(chunk[2].astype(jnp.bfloat16), "x", -1)
    near = hop(chunk[3].astype(jnp.bfloat16), "x", 1)
    both = hop((chunk[1] + passed.astype(jnp.float32)).astype(jnp.bfloat16), "x", -1)
    return (chunk[0] + near.astype(jnp.float32) + both.astype(jnp.float32)).astype(jnp.bfloat16)


def copied_over_tp(at, rows):
    before, after = hop(rows, "x", -1), hop(rows, "x", 1)
    across = hop(before, "x", -1)
    most = other_core(jnp.concatenate([rows, before, after], axis=0))
    return assembled(at, [rows, before, after, across, most, other_core(across)])


def per_device(tokens, norm_gain, gate_weight, up_weight, down_weight):
    at = jnp.stack([lax.axis_index(a) for a in ("zl", "y", "c", "x")]).astype(jnp.int32)
    early, late = gathered(packed(gate_weight, up_weight, down_weight))
    theirs, mine = ffn(at, normalized(tokens, norm_gain), early, late)
    return copied_over_tp(at, summed_over_x(mine, theirs))


def solution(mesh):
    split = Mesh(mesh.devices.reshape(mesh.shape["rep"], 4, 8, 4, 2), ("zh", "zl", "y", "x", "c"))
    tok = P(("zh", "zl", "y"), None)
    fs, tp = ("zl", "y"), ("x", "c")
    placed = (tok, P(), P(fs, tp), P(fs, tp), P(tp, fs))
    return jax.shard_map(per_device, mesh=split, in_specs=placed, out_specs=tok, check_vma=False)
```

```python
import functools

import jax
import jax.numpy as jnp
from jax import lax
from jax.experimental import pallas as pl
from jax.experimental.pallas import tpu as pltpu
from jax.sharding import Mesh
from jax.sharding import PartitionSpec as P


NZ, NY, HID, GU = 4, 8, 704, 1408
D = 2048
HALF = 48
VMEM = pl.BlockSpec(memory_space=pltpu.VMEM)
SMEM = pl.BlockSpec(memory_space=pltpu.SMEM)
ANY = pl.BlockSpec(memory_space=pl.ANY)
RINGS = {"z": (("zh", "zl", "c"), 12), "y": (("y", "c"), 8), "x": (("x", "c"), 4)}


def hop(x, ring, step):
    axes, n = RINGS[ring]
    pairs = [(2 * ((i + (1 - 2 * c) * step) % n) + c, 2 * i + c) for i in range(n) for c in range(2)]
    return lax.ppermute(x, axes, pairs)


def other_core(x):
    return lax.ppermute(x, "c", [(0, 1), (1, 0)])


def pack_kernel(gate_hbm, up_hbm, down_hbm, out_ref, gate_ref, up_ref, down_ref, sems):
    pairs = ((gate_hbm, gate_ref), (up_hbm, up_ref), (down_hbm, down_ref))
    copies = [pltpu.make_async_copy(source, to, sems.at[k]) for k, (source, to) in enumerate(pairs)]
    for copy in copies:
        copy.start()
    for copy in copies:
        copy.wait()

    def pair(at, rows, a_ref, a_at, b_ref, b_at):
        for j in range(5):
            lanes = slice(128 * j, 128 * j + 128)
            out_ref[at : at + rows, 256 * j : 256 * j + 128] = a_ref[a_at : a_at + rows, lanes]
            out_ref[at : at + rows, 256 * j + 128 : 256 * j + 256] = b_ref[b_at : b_at + rows, lanes]
        last = [a_ref[a_at : a_at + rows, 640:704], b_ref[b_at : b_at + rows, 640:704]]
        out_ref[at : at + rows, 1280:1408] = jnp.concatenate(last, axis=1)

    for h in range(2):
        pair(HALF * h, 32, gate_ref, 32 * h, up_ref, 32 * h)
        pair(HALF * h + 32, 16, down_ref, 32 * h, down_ref, 32 * h + 16)


def packed(gate, up, down):
    return pl.pallas_call(
        pack_kernel,
        out_shape=jax.ShapeDtypeStruct((2 * HALF, GU), jnp.bfloat16),
        in_specs=[ANY] * 3,
        out_specs=VMEM,
        scratch_shapes=[pltpu.VMEM((64, HID), jnp.bfloat16)] * 3 + [pltpu.SemaphoreType.DMA((3,))],
        compiler_params=pltpu.CompilerParams(vmem_limit_bytes=63 * 2**20),
        name="pack",
    )(gate, up, down.T)


def norm_kernel(tok_ref, gain_ref, out_ref):
    tok = tok_ref[...].astype(jnp.float32)
    scale = lax.rsqrt(jnp.mean(tok * tok, axis=-1, keepdims=True) + 1e-06)
    normed = tok * scale * gain_ref[...]
    for s in range(16):
        slab = normed[:, 128 * s : 128 * s + 128]
        out_ref[0, s] = slab.astype(jnp.bfloat16)
        out_ref[1, s] = pltpu.roll(slab, 64, 1).astype(jnp.bfloat16)


def normalized(tokens, gain):
    return pl.pallas_call(
        norm_kernel,
        out_shape=jax.ShapeDtypeStruct((2, 16, 512, 128), jnp.bfloat16),
        grid=(8,),
        in_specs=[pl.BlockSpec((64, D), lambda i: (i, 0)), pl.BlockSpec((1, D), lambda i: (0, 0))],
        out_specs=pl.BlockSpec((2, 16, 64, 128), lambda i: (0, 0, i, 0)),
        compiler_params=pltpu.CompilerParams(vmem_limit_bytes=56 * 2**20),
        cost_estimate=pl.CostEstimate(flops=400_000_000, bytes_accessed=6_000_000, transcendentals=512),
        name="norm",
    )(tokens, gain.reshape(1, D))


def gathered(own):
    top, low = own[:HALF], own[HALF:]
    pair = jnp.concatenate([top, hop(top, "z", -2), low, hop(low, "z", 2)], axis=0)

    def whole(dz, dy):
        return [(dz, dy, 0), (dz + 2, dy, 0), (dz, dy, 1), (dz + 2, dy, 1)]

    early, late = [(pair, whole(0, 0))], []
    lo, hi = hop(pair, "y", -1), hop(pair, "y", 1)
    early.append((hop(pair, "z", -1), whole(-1, 0)))
    for k in (1, 2, 3):
        early += [(lo, whole(0, -k)), (hi, whole(0, k))]
        up, down = hop(lo, "z", -1), hop(hi, "z", 1)
        (early if k < 3 else late).extend([(up, whole(-1, -k)), (down, whole(1, k))])
        lo = hop(lo, "y", -1)
        if k < 3:
            hi = hop(hi, "y", 1)
    late += [(lo, whole(0, -4)), (hop(lo, "z", -1), whole(-1, -4))]
    return early, late


def shard_index(at_ref, dz, dy):
    z, y, sign = at_ref[0], at_ref[1], 1 - 2 * at_ref[2]
    return lax.rem(z + sign * dz + 2 * NZ, NZ) * NY + lax.rem(y + sign * dy + 2 * NY, NY)


def place(blocks, places, at_ref, normed_ref, lhs_ref, gu_ref, down_ref):
    low = lax.broadcasted_iota(jnp.int32, (512, 128), 1) < 64
    order = {}
    for block, where in zip(blocks, places):
        for k, (dz, dy, h) in enumerate(where):
            shard = order.setdefault((dz % NZ, dy % NY), len(order))
            index = shard_index(at_ref, dz % NZ, dy % NY)
            at = HALF * k
            gu_ref[64 * shard + 32 * h : 64 * shard + 32 * h + 32, :] = block[at : at + 32, :]
            for part in range(2):
                rows = pl.ds(pl.multiple_of(index * 64 + 32 * h + 16 * part, 16), 16)
                for j in range(5):
                    source = slice(256 * j + 128 * part, 256 * j + 128 * part + 128)
                    down_ref[rows, 128 * j : 128 * j + 128] = block[at + 32 : at + 48, source]
                down_ref[rows, 640:704] = block[at + 32 : at + 48, 1280 + 64 * part : 1344 + 64 * part]
    shards = list(order)
    for j in range(0, len(shards), 2):
        halves = []
        for side in range(2):
            dz, dy = shards[j + side]
            index = shard_index(at_ref, dz, dy)
            odd = lax.rem(index, 2)
            halves.append(normed_ref[odd if side == 0 else 1 - odd, lax.div(index, 2)])
        lhs_ref[:, 64 * j : 64 * j + 128] = jnp.where(low, halves[0], halves[1])


def first_kernel(places, at_ref, normed_ref, *refs):
    blocks = refs[: len(places)]
    pre_ref, down_ref, lhs_ref, gu_ref = refs[len(places) :]
    place(blocks, places, at_ref, normed_ref, lhs_ref, gu_ref, down_ref)
    for j in range(0, GU, 256):
        lanes = slice(j, min(j + 256, GU))
        pre_ref[:, lanes] = jnp.dot(lhs_ref[...], gu_ref[:, lanes], preferred_element_type=jnp.float32)


def last_kernel(places, at_ref, normed_ref, pre_ref, down_in_ref, *refs):
    blocks = refs[: len(places)]
    theirs_ref, mine_ref, down_ref, lhs_ref, gu_ref, hid_ref = refs[len(places) :]
    place(blocks, places, at_ref, normed_ref, lhs_ref, gu_ref, down_ref)
    core, x = at_ref[2], at_ref[3]

    def gated(j, width):
        lanes = slice(256 * j, 256 * j + 2 * width)
        pre = pre_ref[:, lanes] + jnp.dot(lhs_ref[...], gu_ref[:, lanes], preferred_element_type=jnp.float32)
        gate, up = pre[:, :width], pre[:, width:]
        hid = (gate / (1.0 + jnp.exp(-gate)) * up).astype(jnp.bfloat16)
        hid_ref[:, :, 128 * j : 128 * j + width] = hid.reshape(2, 256, width)

    for j in range(5):
        gated(j, 128)
    gated(5, 64)
    for half, out_ref in ((1 - core, theirs_ref), (core, mine_ref)):
        chunks = [lax.rem(x + (1 - 2 * half) * j + 4, 4) for j in range(4)]
        hid = jnp.concatenate([hid_ref[half, pl.ds(pl.multiple_of(64 * c, 64), 64), :] for c in chunks], axis=0)
        for j in range(8):
            rows = slice(256 * j, 256 * j + 256)
            out_ref[:, rows] = lax.dot_general(
                hid, down_ref[rows, :], (((1,), (1,)), ((), ())), preferred_element_type=jnp.float32
            ).astype(jnp.bfloat16)


def shards_of(items):
    return sum(len(where) for _, where in items) // 2


def ffn(at, normed, early, late):
    down_shape = jax.ShapeDtypeStruct((D, HID), jnp.bfloat16)
    k = 64 * shards_of(early)
    pre, down = pl.pallas_call(
        functools.partial(first_kernel, [w for _, w in early]),
        out_shape=(jax.ShapeDtypeStruct((512, GU), jnp.float32), down_shape),
        in_specs=[SMEM] + [VMEM] * (1 + len(early)),
        out_specs=(VMEM, VMEM),
        scratch_shapes=[pltpu.VMEM((512, k), jnp.bfloat16), pltpu.VMEM((k, GU), jnp.bfloat16)],
        compiler_params=pltpu.CompilerParams(vmem_limit_bytes=24 * 2**20),
        cost_estimate=pl.CostEstimate(flops=2 * 512 * k * GU, bytes_accessed=13_000_000, transcendentals=0),
        name="ffn_first",
    )(at, normed, *[a for a, _ in early])
    k = 64 * shards_of(late)
    half = jax.ShapeDtypeStruct((256, D), jnp.bfloat16)
    return pl.pallas_call(
        functools.partial(last_kernel, [w for _, w in late]),
        out_shape=(half, half, down_shape),
        in_specs=[SMEM] + [VMEM] * (3 + len(late)),
        out_specs=(VMEM,) * 3,
        input_output_aliases={3: 2},
        scratch_shapes=[
            pltpu.VMEM((512, k), jnp.bfloat16),
            pltpu.VMEM((k, GU), jnp.bfloat16),
            pltpu.VMEM((2, 256, HID), jnp.bfloat16),
        ],
        compiler_params=pltpu.CompilerParams(vmem_limit_bytes=24 * 2**20),
        cost_estimate=pl.CostEstimate(flops=2_200_000_000, bytes_accessed=10_000_000, transcendentals=360_448),
        name="ffn_last",
    )(at, normed, pre, down, *[a for a, _ in late])[:2]


def assemble_kernel(at_ref, *refs):
    blocks, out_hbm, sems = refs[:-2], refs[-2], refs[-1]
    core, x = at_ref[2], at_ref[3]
    copies = []
    for k, (block, rows) in enumerate(zip(blocks, (64, 64, 64, 64, 192, 64))):
        half = core if k < 4 else 1 - core
        sign = 1 - 2 * half
        steps = ((0,), (-1,), (2,), (1,), (0, -1, 2), (1,))[k]
        for j, step in enumerate(steps):
            row = 256 * half + 64 * lax.rem(x + sign * step + 4, 4)
            to = out_hbm.at[pl.ds(pl.multiple_of(row, 64), 64), :]
            copies.append(pltpu.make_async_copy(block.at[pl.ds(64 * j, 64), :], to, sems.at[len(copies)]))
    for copy in copies:
        copy.start()
    for copy in copies:
        copy.wait()


def assembled(at, blocks):
    return pl.pallas_call(
        assemble_kernel,
        out_shape=jax.ShapeDtypeStruct((512, D), jnp.bfloat16),
        in_specs=[SMEM] + [VMEM] * len(blocks),
        out_specs=ANY,
        scratch_shapes=[pltpu.SemaphoreType.DMA((8,))],
        compiler_params=pltpu.CompilerParams(vmem_limit_bytes=6 * 2**20),
        name="assemble",
    )(at, *blocks)


def summed_over_x(mine, theirs):
    total = mine.astype(jnp.float32) + other_core(theirs).astype(jnp.float32)
    chunk = [total[64 * j : 64 * j + 64] for j in range(4)]
    across = hop(chunk[2].astype(jnp.bfloat16), "x", -2)
    before = hop(chunk[1].astype(jnp.bfloat16), "x", -1)
    after = hop(chunk[3].astype(jnp.bfloat16), "x", 1)
    return (chunk[0] + before + after + across).astype(jnp.bfloat16)


def copied_over_tp(at, rows):
    across = hop(rows, "x", -2)
    before, after = hop(rows, "x", -1), hop(rows, "x", 1)
    most = other_core(jnp.concatenate([rows, before, across], axis=0))
    return assembled(at, [rows, before, across, after, most, other_core(after)])


def per_device(tokens, norm_gain, gate_weight, up_weight, down_weight):
    at = jnp.stack([lax.axis_index(a) for a in ("zl", "y", "c", "x")]).astype(jnp.int32)
    early, late = gathered(packed(gate_weight, up_weight, down_weight))
    theirs, mine = ffn(at, normalized(tokens, norm_gain), early, late)
    return copied_over_tp(at, summed_over_x(mine, theirs))


def solution(mesh):
    split = Mesh(mesh.devices.reshape(mesh.shape["rep"], 4, 8, 4, 2), ("zh", "zl", "y", "x", "c"))
    tok = P(("zh", "zl", "y"), None)
    fs, tp = ("zl", "y"), ("x", "c")
    placed = (tok, P(), P(fs, tp), P(fs, tp), P(tp, fs))
    return jax.shard_map(per_device, mesh=split, in_specs=placed, out_specs=tok, check_vma=False)
```

```python
import functools

import jax
import jax.numpy as jnp
from jax import lax
from jax.experimental import pallas as pl
from jax.experimental.pallas import tpu as pltpu
from jax.sharding import Mesh
from jax.sharding import PartitionSpec as P


NZ, NY, HID, GU = 4, 8, 704, 1408
D = 2048
SHARD = 96
VMEM = pl.BlockSpec(memory_space=pltpu.VMEM)
SMEM = pl.BlockSpec(memory_space=pltpu.SMEM)
ANY = pl.BlockSpec(memory_space=pl.ANY)
RINGS = {"z": (("zh", "zl", "c"), 12), "y": (("y", "c"), 8), "x": (("x", "c"), 4)}


def hop(x, ring, step):
    axes, n = RINGS[ring]
    pairs = [(2 * ((i + (1 - 2 * c) * step) % n) + c, 2 * i + c) for i in range(n) for c in range(2)]
    return lax.ppermute(x, axes, pairs)


def other_core(x):
    return lax.ppermute(x, "c", [(0, 1), (1, 0)])


def pack_kernel(gate_hbm, up_hbm, down_hbm, out_ref, gate_ref, up_ref, down_ref, sems):
    pairs = ((gate_hbm, gate_ref), (up_hbm, up_ref), (down_hbm, down_ref))
    copies = [pltpu.make_async_copy(source, to, sems.at[k]) for k, (source, to) in enumerate(pairs)]
    for copy in copies:
        copy.start()
    for copy in copies:
        copy.wait()

    def pair(at, rows, a_ref, a_at, b_ref, b_at):
        for j in range(5):
            lanes = slice(128 * j, 128 * j + 128)
            out_ref[at : at + rows, 256 * j : 256 * j + 128] = a_ref[a_at : a_at + rows, lanes]
            out_ref[at : at + rows, 256 * j + 128 : 256 * j + 256] = b_ref[b_at : b_at + rows, lanes]
        last = [a_ref[a_at : a_at + rows, 640:704], b_ref[b_at : b_at + rows, 640:704]]
        out_ref[at : at + rows, 1280:1408] = jnp.concatenate(last, axis=1)

    pair(0, 64, gate_ref, 0, up_ref, 0)
    pair(64, 32, down_ref, 0, down_ref, 32)


def packed(gate, up, down):
    return pl.pallas_call(
        pack_kernel,
        out_shape=jax.ShapeDtypeStruct((SHARD, GU), jnp.bfloat16),
        in_specs=[ANY] * 3,
        out_specs=VMEM,
        scratch_shapes=[pltpu.VMEM((64, HID), jnp.bfloat16)] * 3 + [pltpu.SemaphoreType.DMA((3,))],
        compiler_params=pltpu.CompilerParams(vmem_limit_bytes=63 * 2**20),
        name="pack",
    )(gate, up, down.T)


def norm_kernel(tok_ref, gain_ref, out_ref):
    for r in range(0, 512, 64):
        tok = tok_ref[r : r + 64, :].astype(jnp.float32)
        scale = lax.rsqrt(jnp.mean(tok * tok, axis=-1, keepdims=True) + 1e-06)
        normed = tok * scale * gain_ref[...]
        for s in range(16):
            slab = normed[:, 128 * s : 128 * s + 128]
            out_ref[0, s, r : r + 64, :] = slab.astype(jnp.bfloat16)
            out_ref[1, s, r : r + 64, :] = pltpu.roll(slab, 64, 1).astype(jnp.bfloat16)


def normalized(tokens, gain):
    return pl.pallas_call(
        norm_kernel,
        out_shape=jax.ShapeDtypeStruct((2, 16, 512, 128), jnp.bfloat16),
        in_specs=[VMEM] * 2,
        out_specs=VMEM,
        compiler_params=pltpu.CompilerParams(vmem_limit_bytes=8 * 2**20),
        cost_estimate=pl.CostEstimate(flops=400_000_000, bytes_accessed=6_000_000, transcendentals=512),
        name="norm",
    )(tokens, gain.reshape(1, D))


def gathered(own):
    def joined(*items):
        return jnp.concatenate([a for a, _ in items], axis=0), sum((w for _, w in items), [])

    def moved(item, ring, step):
        dz, dy = (step, 0) if ring == "z" else (0, step)
        return hop(item[0], ring, step), [(z + dz, y + dy) for z, y in item[1]]

    def second(item):
        return item[0][SHARD:], item[1][1:]

    own = (own, [(0, 0)])
    far = moved(own, "z", 2)
    lo1, hi1 = moved(own, "y", -1), moved(own, "y", 1)
    lo2 = moved(joined(lo1, far), "y", -1)
    hi2 = moved(joined(hi1, far), "y", 1)
    z1 = moved(joined(own, far, lo1, hi1), "z", -1)
    lo3, hi3 = moved(lo2, "y", -1), moved(hi2, "y", 1)
    z2 = moved(joined(lo2, hi2), "z", -1)
    lo4, hi4 = moved(lo3, "y", -1), moved(second(hi3), "y", 1)
    z3 = moved(joined(lo3, hi3), "z", -1)
    lo5 = moved(second(lo4), "y", -1)
    z4 = moved(joined(lo4, hi4), "z", -1)
    z5 = moved(lo5, "z", -1)
    return [own, far, lo1, hi1, lo2, hi2, z1, lo3, hi3, z2, z3], [lo4, hi4, lo5, z4, z5]


def shard_index(at_ref, dz, dy):
    z, y, sign = at_ref[0], at_ref[1], 1 - 2 * at_ref[2]
    return lax.rem(z + sign * dz + 2 * NZ, NZ) * NY + lax.rem(y + sign * dy + 2 * NY, NY)


def place(blocks, places, at_ref, normed_ref, lhs_ref, gu_ref, down_ref):
    low = lax.broadcasted_iota(jnp.int32, (512, 128), 1) < 64
    shards = []
    for block, where in zip(blocks, places):
        for k, (dz, dy) in enumerate(where):
            index = shard_index(at_ref, dz % NZ, dy % NY)
            at, to = SHARD * k, 64 * len(shards)
            gu_ref[to : to + 64, :] = block[at : at + 64, :]
            for part in range(2):
                rows = pl.ds(pl.multiple_of(index * 64 + 32 * part, 32), 32)
                for j in range(5):
                    source = slice(256 * j + 128 * part, 256 * j + 128 * part + 128)
                    down_ref[rows, 128 * j : 128 * j + 128] = block[at + 64 : at + 96, source]
                down_ref[rows, 640:704] = block[at + 64 : at + 96, 1280 + 64 * part : 1344 + 64 * part]
            shards.append((dz % NZ, dy % NY))
    for j in range(0, len(shards), 2):
        halves = []
        for side in range(2):
            dz, dy = shards[j + side]
            index = shard_index(at_ref, dz, dy)
            odd = lax.rem(index, 2)
            halves.append(normed_ref[odd if side == 0 else 1 - odd, lax.div(index, 2)])
        lhs_ref[:, 64 * j : 64 * j + 128] = jnp.where(low, halves[0], halves[1])


def first_kernel(places, at_ref, normed_ref, *refs):
    blocks = refs[: len(places)]
    pre_ref, down_ref, lhs_ref, gu_ref = refs[len(places) :]
    place(blocks, places, at_ref, normed_ref, lhs_ref, gu_ref, down_ref)
    for j in range(0, GU, 256):
        lanes = slice(j, min(j + 256, GU))
        pre_ref[:, lanes] = jnp.dot(lhs_ref[...], gu_ref[:, lanes], preferred_element_type=jnp.float32)


def last_kernel(places, at_ref, normed_ref, pre_ref, down_in_ref, *refs):
    blocks = refs[: len(places)]
    theirs_ref, mine_ref, down_ref, lhs_ref, gu_ref, hid_ref = refs[len(places) :]
    place(blocks, places, at_ref, normed_ref, lhs_ref, gu_ref, down_ref)
    core, x = at_ref[2], at_ref[3]

    def gated(j, width):
        lanes = slice(256 * j, 256 * j + 2 * width)
        pre = pre_ref[:, lanes] + jnp.dot(lhs_ref[...], gu_ref[:, lanes], preferred_element_type=jnp.float32)
        gate, up = pre[:, :width], pre[:, width:]
        hid = (gate / (1.0 + jnp.exp(-gate)) * up).astype(jnp.bfloat16)
        hid_ref[:, :, 128 * j : 128 * j + width] = hid.reshape(2, 256, width)

    for j in range(5):
        gated(j, 128)
    gated(5, 64)
    for half, out_ref in ((1 - core, theirs_ref), (core, mine_ref)):
        chunks = [lax.rem(x + (1 - 2 * half) * j + 4, 4) for j in range(4)]
        hid = jnp.concatenate([hid_ref[half, pl.ds(pl.multiple_of(64 * c, 64), 64), :] for c in chunks], axis=0)
        for j in range(8):
            rows = slice(256 * j, 256 * j + 256)
            out_ref[:, rows] = lax.dot_general(
                hid, down_ref[rows, :], (((1,), (1,)), ((), ())), preferred_element_type=jnp.float32
            ).astype(jnp.bfloat16)


def shards_of(items):
    return sum(len(where) for _, where in items)


def ffn(at, normed, early, late):
    down_shape = jax.ShapeDtypeStruct((D, HID), jnp.bfloat16)
    k = 64 * shards_of(early)
    pre, down = pl.pallas_call(
        functools.partial(first_kernel, [w for _, w in early]),
        out_shape=(jax.ShapeDtypeStruct((512, GU), jnp.float32), down_shape),
        in_specs=[SMEM] + [VMEM] * (1 + len(early)),
        out_specs=(VMEM, VMEM),
        scratch_shapes=[pltpu.VMEM((512, k), jnp.bfloat16), pltpu.VMEM((k, GU), jnp.bfloat16)],
        compiler_params=pltpu.CompilerParams(vmem_limit_bytes=24 * 2**20),
        cost_estimate=pl.CostEstimate(flops=2 * 512 * k * GU, bytes_accessed=13_000_000, transcendentals=0),
        name="ffn_first",
    )(at, normed, *[a for a, _ in early])
    k = 64 * shards_of(late)
    half = jax.ShapeDtypeStruct((256, D), jnp.bfloat16)
    return pl.pallas_call(
        functools.partial(last_kernel, [w for _, w in late]),
        out_shape=(half, half, down_shape),
        in_specs=[SMEM] + [VMEM] * (3 + len(late)),
        out_specs=(VMEM,) * 3,
        input_output_aliases={3: 2},
        scratch_shapes=[
            pltpu.VMEM((512, k), jnp.bfloat16),
            pltpu.VMEM((k, GU), jnp.bfloat16),
            pltpu.VMEM((2, 256, HID), jnp.bfloat16),
        ],
        compiler_params=pltpu.CompilerParams(vmem_limit_bytes=24 * 2**20),
        cost_estimate=pl.CostEstimate(flops=2_200_000_000, bytes_accessed=10_000_000, transcendentals=360_448),
        name="ffn_last",
    )(at, normed, pre, down, *[a for a, _ in late])[:2]


def assemble_kernel(at_ref, *refs):
    blocks, out_hbm, sems = refs[:-2], refs[-2], refs[-1]
    core, x = at_ref[2], at_ref[3]
    copies = []
    for k, (block, rows) in enumerate(zip(blocks, (64, 64, 64, 64, 192, 64))):
        half = core if k < 4 else 1 - core
        sign = 1 - 2 * half
        steps = ((0,), (-1,), (2,), (1,), (0, -1, 2), (1,))[k]
        for j, step in enumerate(steps):
            row = 256 * half + 64 * lax.rem(x + sign * step + 4, 4)
            to = out_hbm.at[pl.ds(pl.multiple_of(row, 64), 64), :]
            copies.append(pltpu.make_async_copy(block.at[pl.ds(64 * j, 64), :], to, sems.at[len(copies)]))
    for copy in copies:
        copy.start()
    for copy in copies:
        copy.wait()


def assembled(at, blocks):
    return pl.pallas_call(
        assemble_kernel,
        out_shape=jax.ShapeDtypeStruct((512, D), jnp.bfloat16),
        in_specs=[SMEM] + [VMEM] * len(blocks),
        out_specs=ANY,
        scratch_shapes=[pltpu.SemaphoreType.DMA((8,))],
        compiler_params=pltpu.CompilerParams(vmem_limit_bytes=6 * 2**20),
        name="assemble",
    )(at, *blocks)


def summed_over_x(mine, theirs):
    total = mine.astype(jnp.float32) + other_core(theirs).astype(jnp.float32)
    chunk = [total[64 * j : 64 * j + 64] for j in range(4)]
    across = hop(chunk[2].astype(jnp.bfloat16), "x", -2)
    before = hop(chunk[1].astype(jnp.bfloat16), "x", -1)
    after = hop(chunk[3].astype(jnp.bfloat16), "x", 1)
    return (chunk[0] + before + after + across).astype(jnp.bfloat16)


def copied_over_tp(at, rows):
    across = hop(rows, "x", -2)
    before, after = hop(rows, "x", -1), hop(rows, "x", 1)
    most = other_core(jnp.concatenate([rows, before, across], axis=0))
    return assembled(at, [rows, before, across, after, most, other_core(after)])


def per_device(tokens, norm_gain, gate_weight, up_weight, down_weight):
    at = jnp.stack([lax.axis_index(a) for a in ("zl", "y", "c", "x")]).astype(jnp.int32)
    early, late = gathered(packed(gate_weight, up_weight, down_weight))
    theirs, mine = ffn(at, normalized(tokens, norm_gain), early, late)
    return copied_over_tp(at, summed_over_x(mine, theirs))


def solution(mesh):
    split = Mesh(mesh.devices.reshape(mesh.shape["rep"], 4, 8, 4, 2), ("zh", "zl", "y", "x", "c"))
    tok = P(("zh", "zl", "y"), None)
    fs, tp = ("zl", "y"), ("x", "c")
    placed = (tok, P(), P(fs, tp), P(fs, tp), P(tp, fs))
    return jax.shard_map(per_device, mesh=split, in_specs=placed, out_specs=tok, check_vma=False)
```

```python
import functools

import jax
import jax.numpy as jnp
from jax import lax
from jax.experimental import pallas as pl
from jax.experimental.pallas import tpu as pltpu
from jax.sharding import Mesh
from jax.sharding import PartitionSpec as P


NZ, NY, HID, GU = 4, 8, 704, 1408
D = 2048
SHARD = 96
VMEM = pl.BlockSpec(memory_space=pltpu.VMEM)
SMEM = pl.BlockSpec(memory_space=pltpu.SMEM)
ANY = pl.BlockSpec(memory_space=pl.ANY)
RINGS = {"z": (("zh", "zl", "c"), 12), "y": (("y", "c"), 8), "x": (("x", "c"), 4)}


def hop(x, ring, step):
    axes, n = RINGS[ring]
    pairs = [(2 * ((i + (1 - 2 * c) * step) % n) + c, 2 * i + c) for i in range(n) for c in range(2)]
    return lax.ppermute(x, axes, pairs)


def trade(x, first):
    flip = (1, 3) if first else (3, 1)
    return lax.ppermute(x, ("x", "c"), [(2 * (i ^ flip[c]) + c, 2 * i + c) for i in range(4) for c in range(2)])


def partners(x, core):
    return [x, lax.bitwise_xor(x, 3 - 2 * core), lax.bitwise_xor(x, 1 + 2 * core), lax.bitwise_xor(x, 2)]


def other_core(x):
    return lax.ppermute(x, "c", [(0, 1), (1, 0)])


def pack_kernel(gate_hbm, up_hbm, down_hbm, out_ref, gate_ref, up_ref, down_ref, sems):
    pairs = ((gate_hbm, gate_ref), (up_hbm, up_ref), (down_hbm, down_ref))
    copies = [pltpu.make_async_copy(source, to, sems.at[k]) for k, (source, to) in enumerate(pairs)]
    for copy in copies:
        copy.start()
    for copy in copies:
        copy.wait()

    def pair(at, rows, a_ref, a_at, b_ref, b_at):
        for j in range(5):
            lanes = slice(128 * j, 128 * j + 128)
            out_ref[at : at + rows, 256 * j : 256 * j + 128] = a_ref[a_at : a_at + rows, lanes]
            out_ref[at : at + rows, 256 * j + 128 : 256 * j + 256] = b_ref[b_at : b_at + rows, lanes]
        last = [a_ref[a_at : a_at + rows, 640:704], b_ref[b_at : b_at + rows, 640:704]]
        out_ref[at : at + rows, 1280:1408] = jnp.concatenate(last, axis=1)

    pair(0, 64, gate_ref, 0, up_ref, 0)
    pair(64, 32, down_ref, 0, down_ref, 32)


def packed(gate, up, down):
    return pl.pallas_call(
        pack_kernel,
        out_shape=jax.ShapeDtypeStruct((SHARD, GU), jnp.bfloat16),
        in_specs=[ANY] * 3,
        out_specs=VMEM,
        scratch_shapes=[pltpu.VMEM((64, HID), jnp.bfloat16)] * 3 + [pltpu.SemaphoreType.DMA((3,))],
        compiler_params=pltpu.CompilerParams(vmem_limit_bytes=63 * 2**20),
        name="pack",
    )(gate, up, down.T)


def norm_kernel(tok_ref, gain_ref, out_ref):
    for r in range(0, 512, 64):
        tok = tok_ref[r : r + 64, :].astype(jnp.float32)
        scale = lax.rsqrt(jnp.mean(tok * tok, axis=-1, keepdims=True) + 1e-06)
        normed = tok * scale * gain_ref[...]
        for s in range(16):
            slab = normed[:, 128 * s : 128 * s + 128]
            out_ref[0, s, r : r + 64, :] = slab.astype(jnp.bfloat16)
            out_ref[1, s, r : r + 64, :] = pltpu.roll(slab, 64, 1).astype(jnp.bfloat16)


def normalized(tokens, gain):
    return pl.pallas_call(
        norm_kernel,
        out_shape=jax.ShapeDtypeStruct((2, 16, 512, 128), jnp.bfloat16),
        in_specs=[VMEM] * 2,
        out_specs=VMEM,
        compiler_params=pltpu.CompilerParams(vmem_limit_bytes=8 * 2**20),
        cost_estimate=pl.CostEstimate(flops=400_000_000, bytes_accessed=6_000_000, transcendentals=512),
        name="norm",
    )(tokens, gain.reshape(1, D))


def gathered(own):
    def whole(dz, dy):
        return [(dz, dy), (dz + 2, dy)]

    pair = jnp.concatenate([own, hop(own, "z", 2)], axis=0)
    early, late = [(pair, whole(0, 0))], []
    lo, hi = hop(pair, "y", -1), hop(pair, "y", 1)
    early.append((hop(pair, "z", -1), whole(-1, 0)))
    for k in (1, 2, 3):
        early += [(lo, whole(0, -k)), (hi, whole(0, k))]
        up, down = hop(lo, "z", -1), hop(hi, "z", 1)
        (early if k < 3 else late).extend([(up, whole(-1, -k)), (down, whole(1, k))])
        lo = hop(lo, "y", -1)
        if k < 3:
            hi = hop(hi, "y", 1)
    late += [(lo, whole(0, -4)), (hop(lo, "z", -1), whole(-1, -4))]
    return early, late


def shard_index(at_ref, dz, dy):
    z, y, sign = at_ref[0], at_ref[1], 1 - 2 * at_ref[2]
    return lax.rem(z + sign * dz + 2 * NZ, NZ) * NY + lax.rem(y + sign * dy + 2 * NY, NY)


def place(blocks, places, at_ref, normed_ref, lhs_ref, gu_ref, down_ref):
    low = lax.broadcasted_iota(jnp.int32, (512, 128), 1) < 64
    shards = []
    for block, where in zip(blocks, places):
        for k, (dz, dy) in enumerate(where):
            index = shard_index(at_ref, dz % NZ, dy % NY)
            at, to = SHARD * k, 64 * len(shards)
            gu_ref[to : to + 64, :] = block[at : at + 64, :]
            for part in range(2):
                rows = pl.ds(pl.multiple_of(index * 64 + 32 * part, 32), 32)
                for j in range(5):
                    source = slice(256 * j + 128 * part, 256 * j + 128 * part + 128)
                    down_ref[rows, 128 * j : 128 * j + 128] = block[at + 64 : at + 96, source]
                down_ref[rows, 640:704] = block[at + 64 : at + 96, 1280 + 64 * part : 1344 + 64 * part]
            shards.append((dz % NZ, dy % NY))
    for j in range(0, len(shards), 2):
        halves = []
        for side in range(2):
            dz, dy = shards[j + side]
            index = shard_index(at_ref, dz, dy)
            odd = lax.rem(index, 2)
            halves.append(normed_ref[odd if side == 0 else 1 - odd, lax.div(index, 2)])
        lhs_ref[:, 64 * j : 64 * j + 128] = jnp.where(low, halves[0], halves[1])


def first_kernel(places, at_ref, normed_ref, *refs):
    blocks = refs[: len(places)]
    pre_ref, down_ref, lhs_ref, gu_ref = refs[len(places) :]
    place(blocks, places, at_ref, normed_ref, lhs_ref, gu_ref, down_ref)
    for j in range(0, GU, 256):
        lanes = slice(j, min(j + 256, GU))
        pre_ref[:, lanes] = jnp.dot(lhs_ref[...], gu_ref[:, lanes], preferred_element_type=jnp.float32)


def down_product(hid_ref, down_ref, half, x, out_ref):
    rows = [pl.ds(pl.multiple_of(64 * c, 64), 64) for c in partners(x, half)]
    hid = jnp.concatenate([hid_ref[half, r, :] for r in rows], axis=0)
    for j in range(8):
        lanes = slice(256 * j, 256 * j + 256)
        out_ref[:, lanes] = lax.dot_general(
            hid, down_ref[lanes, :], (((1,), (1,)), ((), ())), preferred_element_type=jnp.float32
        ).astype(jnp.bfloat16)


def last_kernel(places, at_ref, normed_ref, pre_ref, down_in_ref, *refs):
    blocks = refs[: len(places)]
    theirs_ref, hid_ref, down_ref, lhs_ref, gu_ref = refs[len(places) :]
    place(blocks, places, at_ref, normed_ref, lhs_ref, gu_ref, down_ref)

    def gated(j, width):
        lanes = slice(256 * j, 256 * j + 2 * width)
        pre = pre_ref[:, lanes] + jnp.dot(lhs_ref[...], gu_ref[:, lanes], preferred_element_type=jnp.float32)
        gate, up = pre[:, :width], pre[:, width:]
        hid = (gate / (1.0 + jnp.exp(-gate)) * up).astype(jnp.bfloat16)
        hid_ref[:, :, 128 * j : 128 * j + width] = hid.reshape(2, 256, width)

    for j in range(5):
        gated(j, 128)
    gated(5, 64)
    down_product(hid_ref, down_ref, 1 - at_ref[2], at_ref[3], theirs_ref)


def mine_kernel(at_ref, hid_ref, down_ref, mine_ref):
    down_product(hid_ref, down_ref, at_ref[2], at_ref[3], mine_ref)


def shards_of(items):
    return sum(len(where) for _, where in items)


def ffn(at, normed, early, late):
    down_shape = jax.ShapeDtypeStruct((D, HID), jnp.bfloat16)
    k = 64 * shards_of(early)
    pre, down = pl.pallas_call(
        functools.partial(first_kernel, [w for _, w in early]),
        out_shape=(jax.ShapeDtypeStruct((512, GU), jnp.float32), down_shape),
        in_specs=[SMEM] + [VMEM] * (1 + len(early)),
        out_specs=(VMEM, VMEM),
        scratch_shapes=[pltpu.VMEM((512, k), jnp.bfloat16), pltpu.VMEM((k, GU), jnp.bfloat16)],
        compiler_params=pltpu.CompilerParams(vmem_limit_bytes=24 * 2**20),
        cost_estimate=pl.CostEstimate(flops=2 * 512 * k * GU, bytes_accessed=13_000_000, transcendentals=0),
        name="ffn_first",
    )(at, normed, *[a for a, _ in early])
    k = 64 * shards_of(late)
    half = jax.ShapeDtypeStruct((256, D), jnp.bfloat16)
    theirs, hid, down = pl.pallas_call(
        functools.partial(last_kernel, [w for _, w in late]),
        out_shape=(half, jax.ShapeDtypeStruct((2, 256, HID), jnp.bfloat16), down_shape),
        in_specs=[SMEM] + [VMEM] * (3 + len(late)),
        out_specs=(VMEM,) * 3,
        input_output_aliases={3: 2},
        scratch_shapes=[pltpu.VMEM((512, k), jnp.bfloat16), pltpu.VMEM((k, GU), jnp.bfloat16)],
        compiler_params=pltpu.CompilerParams(vmem_limit_bytes=24 * 2**20),
        cost_estimate=pl.CostEstimate(flops=1_480_000_000, bytes_accessed=10_000_000, transcendentals=360_448),
        name="ffn_last",
    )(at, normed, pre, down, *[a for a, _ in late])
    mine = pl.pallas_call(
        mine_kernel,
        out_shape=half,
        in_specs=[SMEM] + [VMEM] * 2,
        out_specs=VMEM,
        compiler_params=pltpu.CompilerParams(vmem_limit_bytes=12 * 2**20),
        cost_estimate=pl.CostEstimate(flops=740_000_000, bytes_accessed=5_000_000, transcendentals=0),
        name="ffn_mine",
    )(at, hid, down)
    return theirs, mine


def assemble_kernel(owners, at_ref, *refs):
    out_hbm, sems = refs[-2:]
    core, x = at_ref[2], at_ref[3]
    copies = []
    for (near, slots), block in zip(owners, refs):
        half = core if near else 1 - core
        for j, slot in enumerate(slots):
            row = pl.multiple_of(256 * half + 64 * partners(x, half)[slot], 64)
            to = out_hbm.at[pl.ds(row, 64), :]
            copies.append(pltpu.make_async_copy(block.at[pl.ds(64 * j, 64), :], to, sems.at[len(copies)]))
    for copy in copies:
        copy.start()
    for copy in copies:
        copy.wait()


def assembled(at, blocks, owners, into):
    aliased = [] if into is None else [into]
    return pl.pallas_call(
        functools.partial(assemble_kernel, owners),
        out_shape=jax.ShapeDtypeStruct((512, D), jnp.bfloat16),
        in_specs=[SMEM] + [VMEM] * len(blocks) + [ANY] * len(aliased),
        out_specs=ANY,
        input_output_aliases={1 + len(blocks): 0} if aliased else {},
        scratch_shapes=[pltpu.SemaphoreType.DMA((2 * len(blocks),))],
        compiler_params=pltpu.CompilerParams(vmem_limit_bytes=6 * 2**20),
        cost_estimate=pl.CostEstimate(flops=200_000_000, bytes_accessed=2_000_000, transcendentals=0),
    )(at, *blocks, *aliased)


def summed_over_x(mine, theirs):
    got = other_core(theirs)
    total = mine.astype(jnp.float32) + got.astype(jnp.float32)
    two = total[:128] + trade(total[128:].astype(jnp.bfloat16), True)
    return (two[:64] + trade(two[64:].astype(jnp.bfloat16), False)).astype(jnp.bfloat16)


def copied_over_tp(at, rows):
    two = jnp.concatenate([rows, trade(rows, False)], axis=0)
    rest = trade(two, True)
    far_two = other_core(two)
    far_rest = other_core(rest)
    owners = [(True, (0, 1)), (True, (2, 3)), (False, (0, 1))]
    most = assembled(at, [two, rest, far_two], owners, None)
    return assembled(at, [far_rest], [(False, (2, 3))], most)


def per_device(tokens, norm_gain, gate_weight, up_weight, down_weight):
    at = jnp.stack([lax.axis_index(a) for a in ("zl", "y", "c", "x")]).astype(jnp.int32)
    early, late = gathered(packed(gate_weight, up_weight, down_weight))
    theirs, mine = ffn(at, normalized(tokens, norm_gain), early, late)
    return copied_over_tp(at, summed_over_x(mine, theirs))


def solution(mesh):
    split = Mesh(mesh.devices.reshape(mesh.shape["rep"], 4, 8, 4, 2), ("zh", "zl", "y", "x", "c"))
    tok = P(("zh", "zl", "y"), None)
    fs, tp = ("zl", "y"), ("x", "c")
    placed = (tok, P(), P(fs, tp), P(fs, tp), P(tp, fs))
    return jax.shard_map(per_device, mesh=split, in_specs=placed, out_specs=tok, check_vma=False)
```

```python
import functools

import jax
import jax.numpy as jnp
from jax import lax
from jax.experimental import pallas as pl
from jax.experimental.pallas import tpu as pltpu
from jax.sharding import Mesh
from jax.sharding import PartitionSpec as P


NZ, NY, HID, GU = 4, 8, 704, 1408
D = 2048
SHARD = 96
VMEM = pl.BlockSpec(memory_space=pltpu.VMEM)
ANY = pl.BlockSpec(memory_space=pl.ANY)
RINGS = {"z": (("zh", "zl", "c"), 12), "y": (("y", "c"), 8), "x": (("x", "c"), 4)}


def hop(x, ring, step):
    axes, n = RINGS[ring]
    pairs = [(2 * ((i + (1 - 2 * c) * step) % n) + c, 2 * i + c) for i in range(n) for c in range(2)]
    return lax.ppermute(x, axes, pairs)


def other_core(x):
    return lax.ppermute(x, "c", [(0, 1), (1, 0)])


def pack_kernel(gate_hbm, up_hbm, down_hbm, out_ref, gate_ref, up_ref, down_ref, sems):
    pairs = ((gate_hbm, gate_ref), (up_hbm, up_ref), (down_hbm, down_ref))
    copies = [pltpu.make_async_copy(source, to, sems.at[k]) for k, (source, to) in enumerate(pairs)]
    for copy in copies:
        copy.start()
    for copy in copies:
        copy.wait()

    def pair(at, rows, a_ref, a_at, b_ref, b_at):
        for j in range(5):
            lanes = slice(128 * j, 128 * j + 128)
            out_ref[at : at + rows, 256 * j : 256 * j + 128] = a_ref[a_at : a_at + rows, lanes]
            out_ref[at : at + rows, 256 * j + 128 : 256 * j + 256] = b_ref[b_at : b_at + rows, lanes]
        last = [a_ref[a_at : a_at + rows, 640:704], b_ref[b_at : b_at + rows, 640:704]]
        out_ref[at : at + rows, 1280:1408] = jnp.concatenate(last, axis=1)

    pair(0, 64, gate_ref, 0, up_ref, 0)
    pair(64, 32, down_ref, 0, down_ref, 32)


def packed(gate, up, down):
    return pl.pallas_call(
        pack_kernel,
        out_shape=jax.ShapeDtypeStruct((SHARD, GU), jnp.bfloat16),
        in_specs=[ANY] * 3,
        out_specs=VMEM,
        scratch_shapes=[pltpu.VMEM((64, HID), jnp.bfloat16)] * 3 + [pltpu.SemaphoreType.DMA((3,))],
        compiler_params=pltpu.CompilerParams(vmem_limit_bytes=63 * 2**20),
        name="pack",
    )(gate, up, down.T)


def norm_kernel(tok_ref, gain_ref, out_ref):
    for r in range(0, 512, 64):
        tok = tok_ref[r : r + 64, :].astype(jnp.float32)
        scale = lax.rsqrt(jnp.mean(tok * tok, axis=-1, keepdims=True) + 1e-06)
        normed = tok * scale * gain_ref[...]
        for s in range(16):
            slab = normed[:, 128 * s : 128 * s + 128]
            out_ref[0, s, r : r + 64, :] = slab.astype(jnp.bfloat16)
            out_ref[1, s, r : r + 64, :] = pltpu.roll(slab, 64, 1).astype(jnp.bfloat16)


def normalized(tokens, gain):
    return pl.pallas_call(
        norm_kernel,
        out_shape=jax.ShapeDtypeStruct((2, 16, 512, 128), jnp.bfloat16),
        in_specs=[VMEM] * 2,
        out_specs=VMEM,
        compiler_params=pltpu.CompilerParams(vmem_limit_bytes=8 * 2**20),
        cost_estimate=pl.CostEstimate(flops=400_000_000, bytes_accessed=6_000_000, transcendentals=512),
        name="norm",
    )(tokens, gain.reshape(1, D))


def gathered(own):
    def whole(dz, dy):
        return [(dz, dy), (dz + 2, dy)]

    pair = jnp.concatenate([own, hop(own, "z", 2)], axis=0)
    early, late = [(pair, whole(0, 0))], []
    lo, hi = hop(pair, "y", -1), hop(pair, "y", 1)
    early.append((hop(pair, "z", -1), whole(-1, 0)))
    for k in (1, 2, 3):
        early += [(lo, whole(0, -k)), (hi, whole(0, k))]
        up, down = hop(lo, "z", -1), hop(hi, "z", 1)
        (early if k < 3 else late).extend([(up, whole(-1, -k)), (down, whole(1, k))])
        lo = hop(lo, "y", -1)
        if k < 3:
            hi = hop(hi, "y", 1)
    late += [(lo, whole(0, -4)), (hop(lo, "z", -1), whole(-1, -4))]
    return early, late


def shard_index(dz, dy):
    z, y, sign = lax.axis_index("zl"), lax.axis_index("y"), 1 - 2 * lax.axis_index("c")
    return lax.rem(z + sign * dz + 2 * NZ, NZ) * NY + lax.rem(y + sign * dy + 2 * NY, NY)


def place(blocks, places, normed_ref, lhs_ref, gu_ref, down_ref):
    low = lax.broadcasted_iota(jnp.int32, (512, 128), 1) < 64
    shards = []
    for block, where in zip(blocks, places):
        for k, (dz, dy) in enumerate(where):
            index = shard_index(dz % NZ, dy % NY)
            at, to = SHARD * k, 64 * len(shards)
            gu_ref[to : to + 64, :] = block[at : at + 64, :]
            for part in range(2):
                rows = pl.ds(pl.multiple_of(index * 64 + 32 * part, 32), 32)
                for j in range(5):
                    source = slice(256 * j + 128 * part, 256 * j + 128 * part + 128)
                    down_ref[rows, 128 * j : 128 * j + 128] = block[at + 64 : at + 96, source]
                down_ref[rows, 640:704] = block[at + 64 : at + 96, 1280 + 64 * part : 1344 + 64 * part]
            shards.append((dz % NZ, dy % NY))
    for j in range(0, len(shards), 2):
        halves = []
        for side in range(2):
            dz, dy = shards[j + side]
            index = shard_index(dz, dy)
            odd = lax.rem(index, 2)
            halves.append(normed_ref[odd if side == 0 else 1 - odd, lax.div(index, 2)])
        lhs_ref[:, 64 * j : 64 * j + 128] = jnp.where(low, halves[0], halves[1])


def first_kernel(places, normed_ref, *refs):
    blocks = refs[: len(places)]
    pre_ref, down_ref, lhs_ref, gu_ref = refs[len(places) :]
    place(blocks, places, normed_ref, lhs_ref, gu_ref, down_ref)
    for j in range(0, GU, 256):
        lanes = slice(j, min(j + 256, GU))
        pre_ref[:, lanes] = jnp.dot(lhs_ref[...], gu_ref[:, lanes], preferred_element_type=jnp.float32)


def down_product(hid_ref, down_ref, half, out_ref):
    x = lax.axis_index("x")
    rows = [pl.ds(pl.multiple_of(64 * lax.rem(x + (1 - 2 * half) * j + 4, 4), 64), 64) for j in range(4)]
    hid = jnp.concatenate([hid_ref[half, r, :] for r in rows], axis=0)
    for j in range(8):
        lanes = slice(256 * j, 256 * j + 256)
        out_ref[:, lanes] = lax.dot_general(
            hid, down_ref[lanes, :], (((1,), (1,)), ((), ())), preferred_element_type=jnp.float32
        ).astype(jnp.bfloat16)


def last_kernel(places, normed_ref, pre_ref, down_in_ref, *refs):
    blocks = refs[: len(places)]
    theirs_ref, hid_ref, down_ref, lhs_ref, gu_ref = refs[len(places) :]
    place(blocks, places, normed_ref, lhs_ref, gu_ref, down_ref)

    def gated(j, width):
        lanes = slice(256 * j, 256 * j + 2 * width)
        pre = pre_ref[:, lanes] + jnp.dot(lhs_ref[...], gu_ref[:, lanes], preferred_element_type=jnp.float32)
        gate, up = pre[:, :width], pre[:, width:]
        hid = (gate / (1.0 + jnp.exp(-gate)) * up).astype(jnp.bfloat16)
        hid_ref[:, :, 128 * j : 128 * j + width] = hid.reshape(2, 256, width)

    for j in range(5):
        gated(j, 128)
    gated(5, 64)
    down_product(hid_ref, down_ref, 1 - lax.axis_index("c"), theirs_ref)


def mine_kernel(hid_ref, down_ref, mine_ref):
    down_product(hid_ref, down_ref, lax.axis_index("c"), mine_ref)


def shards_of(items):
    return sum(len(where) for _, where in items)


def ffn(normed, early, late):
    down_shape = jax.ShapeDtypeStruct((D, HID), jnp.bfloat16)
    k = 64 * shards_of(early)
    pre, down = pl.pallas_call(
        functools.partial(first_kernel, [w for _, w in early]),
        out_shape=(jax.ShapeDtypeStruct((512, GU), jnp.float32), down_shape),
        in_specs=[VMEM] * (1 + len(early)),
        out_specs=(VMEM, VMEM),
        scratch_shapes=[pltpu.VMEM((512, k), jnp.bfloat16), pltpu.VMEM((k, GU), jnp.bfloat16)],
        compiler_params=pltpu.CompilerParams(vmem_limit_bytes=24 * 2**20),
        cost_estimate=pl.CostEstimate(flops=2 * 512 * k * GU, bytes_accessed=13_000_000, transcendentals=0),
        name="ffn_first",
    )(normed, *[a for a, _ in early])
    k = 64 * shards_of(late)
    half = jax.ShapeDtypeStruct((256, D), jnp.bfloat16)
    theirs, hid, down = pl.pallas_call(
        functools.partial(last_kernel, [w for _, w in late]),
        out_shape=(half, jax.ShapeDtypeStruct((2, 256, HID), jnp.bfloat16), down_shape),
        in_specs=[VMEM] * (3 + len(late)),
        out_specs=(VMEM,) * 3,
        input_output_aliases={2: 2},
        scratch_shapes=[pltpu.VMEM((512, k), jnp.bfloat16), pltpu.VMEM((k, GU), jnp.bfloat16)],
        compiler_params=pltpu.CompilerParams(vmem_limit_bytes=24 * 2**20),
        cost_estimate=pl.CostEstimate(flops=1_480_000_000, bytes_accessed=10_000_000, transcendentals=360_448),
        name="ffn_last",
    )(normed, pre, down, *[a for a, _ in late])
    mine = pl.pallas_call(
        mine_kernel,
        out_shape=half,
        in_specs=[VMEM] * 2,
        out_specs=VMEM,
        compiler_params=pltpu.CompilerParams(vmem_limit_bytes=12 * 2**20),
        cost_estimate=pl.CostEstimate(flops=740_000_000, bytes_accessed=5_000_000, transcendentals=0),
        name="ffn_mine",
    )(hid, down)
    return theirs, mine


def assemble_kernel(*refs):
    blocks, out_hbm, sems = refs[:-2], refs[-2], refs[-1]
    core, x = lax.axis_index("c"), lax.axis_index("x")
    copies = []
    for k, (block, rows) in enumerate(zip(blocks, (64, 64, 64, 64, 192, 64))):
        half = core if k < 4 else 1 - core
        sign = 1 - 2 * half
        steps = ((0,), (-1,), (2,), (1,), (0, -1, 2), (1,))[k]
        for j, step in enumerate(steps):
            row = 256 * half + 64 * lax.rem(x + sign * step + 4, 4)
            to = out_hbm.at[pl.ds(pl.multiple_of(row, 64), 64), :]
            copies.append(pltpu.make_async_copy(block.at[pl.ds(64 * j, 64), :], to, sems.at[len(copies)]))
    for copy in copies:
        copy.start()
    for copy in copies:
        copy.wait()


def assembled(blocks):
    return pl.pallas_call(
        assemble_kernel,
        out_shape=jax.ShapeDtypeStruct((512, D), jnp.bfloat16),
        in_specs=[VMEM] * len(blocks),
        out_specs=ANY,
        scratch_shapes=[pltpu.SemaphoreType.DMA((8,))],
        compiler_params=pltpu.CompilerParams(vmem_limit_bytes=6 * 2**20),
        name="assemble",
    )(*blocks)


def summed_over_x(mine, theirs):
    total = mine.astype(jnp.float32) + other_core(theirs).astype(jnp.float32)
    chunk = [total[64 * j : 64 * j + 64] for j in range(4)]
    across = hop(chunk[2].astype(jnp.bfloat16), "x", -2)
    before = hop(chunk[1].astype(jnp.bfloat16), "x", -1)
    after = hop(chunk[3].astype(jnp.bfloat16), "x", 1)
    return (chunk[0] + before + after + across).astype(jnp.bfloat16)


def copied_over_tp(rows):
    across = hop(rows, "x", -2)
    before, after = hop(rows, "x", -1), hop(rows, "x", 1)
    most = other_core(jnp.concatenate([rows, before, across], axis=0))
    return assembled([rows, before, across, after, most, other_core(after)])


def per_device(tokens, norm_gain, gate_weight, up_weight, down_weight):
    early, late = gathered(packed(gate_weight, up_weight, down_weight))
    theirs, mine = ffn(normalized(tokens, norm_gain), early, late)
    return copied_over_tp(summed_over_x(mine, theirs))


def solution(mesh):
    split = Mesh(mesh.devices.reshape(mesh.shape["rep"], 4, 8, 4, 2), ("zh", "zl", "y", "x", "c"))
    tok = P(("zh", "zl", "y"), None)
    fs, tp = ("zl", "y"), ("x", "c")
    placed = (tok, P(), P(fs, tp), P(fs, tp), P(tp, fs))
    return jax.shard_map(per_device, mesh=split, in_specs=placed, out_specs=tok, check_vma=False)
```

```python
import functools

import jax
import jax.numpy as jnp
from jax import lax
from jax.experimental import pallas as pl
from jax.experimental.pallas import tpu as pltpu
from jax.sharding import Mesh
from jax.sharding import PartitionSpec as P


NZ, NY, HID, GU = 4, 8, 704, 1408
D = 2048
SHARD = 96
VMEM = pl.BlockSpec(memory_space=pltpu.VMEM)
ANY = pl.BlockSpec(memory_space=pl.ANY)
RINGS = {"z": (("zh", "zl", "c"), 12), "y": (("y", "c"), 8), "x": (("x", "c"), 4)}


def hop(x, ring, step):
    axes, n = RINGS[ring]
    pairs = [(2 * ((i + (1 - 2 * c) * step) % n) + c, 2 * i + c) for i in range(n) for c in range(2)]
    return lax.ppermute(x, axes, pairs)


def other_core(x):
    return lax.ppermute(x, "c", [(0, 1), (1, 0)])


def pack_kernel(gate_hbm, up_hbm, down_hbm, out_ref, gate_ref, up_ref, down_ref, sems):
    pairs = ((gate_hbm, gate_ref), (up_hbm, up_ref), (down_hbm, down_ref))
    copies = [pltpu.make_async_copy(source, to, sems.at[k]) for k, (source, to) in enumerate(pairs)]
    for copy in copies:
        copy.start()
    for copy in copies:
        copy.wait()

    def pair(at, rows, a_ref, a_at, b_ref, b_at):
        for j in range(5):
            lanes = slice(128 * j, 128 * j + 128)
            out_ref[at : at + rows, 256 * j : 256 * j + 128] = a_ref[a_at : a_at + rows, lanes]
            out_ref[at : at + rows, 256 * j + 128 : 256 * j + 256] = b_ref[b_at : b_at + rows, lanes]
        last = [a_ref[a_at : a_at + rows, 640:704], b_ref[b_at : b_at + rows, 640:704]]
        out_ref[at : at + rows, 1280:1408] = jnp.concatenate(last, axis=1)

    pair(0, 64, gate_ref, 0, up_ref, 0)
    pair(64, 32, down_ref, 0, down_ref, 32)


def packed(gate, up, down):
    return pl.pallas_call(
        pack_kernel,
        out_shape=jax.ShapeDtypeStruct((SHARD, GU), jnp.bfloat16),
        in_specs=[ANY] * 3,
        out_specs=VMEM,
        scratch_shapes=[pltpu.VMEM((64, HID), jnp.bfloat16)] * 3 + [pltpu.SemaphoreType.DMA((3,))],
        compiler_params=pltpu.CompilerParams(vmem_limit_bytes=63 * 2**20),
        name="pack",
    )(gate, up, down.T)


def norm_kernel(tok_ref, gain_ref, out_ref):
    for r in range(0, 512, 64):
        tok = tok_ref[r : r + 64, :].astype(jnp.float32)
        scale = lax.rsqrt(jnp.mean(tok * tok, axis=-1, keepdims=True) + 1e-06)
        normed = tok * scale * gain_ref[...]
        for s in range(16):
            slab = normed[:, 128 * s : 128 * s + 128]
            out_ref[0, s, r : r + 64, :] = slab.astype(jnp.bfloat16)
            out_ref[1, s, r : r + 64, :] = pltpu.roll(slab, 64, 1).astype(jnp.bfloat16)


def normalized(tokens, gain):
    return pl.pallas_call(
        norm_kernel,
        out_shape=jax.ShapeDtypeStruct((2, 16, 512, 128), jnp.bfloat16),
        in_specs=[VMEM] * 2,
        out_specs=VMEM,
        compiler_params=pltpu.CompilerParams(vmem_limit_bytes=8 * 2**20),
        cost_estimate=pl.CostEstimate(flops=400_000_000, bytes_accessed=6_000_000, transcendentals=512),
        name="norm",
    )(tokens, gain.reshape(1, D))


def gathered(own):
    near, far = [own], [hop(own, "z", -2)]
    for _ in range(1, NY):
        near.append(hop(near[-1], "y", -1))
        far.append(hop(far[-1], "y", -1))
    early, late = [], []
    for k in range(NY):
        (late if k == 7 else early).append((near[k], [(0, -k)]))
        (late if k >= 6 else early).append((far[k], [(2, -k)]))
        (late if k >= 6 else early).append((hop(near[k], "z", -1), [(-1, -k)]))
        (late if k >= 5 else early).append((hop(far[k], "z", -1), [(1, -k)]))
    return early, late


def shard_index(dz, dy):
    z, y, sign = lax.axis_index("zl"), lax.axis_index("y"), 1 - 2 * lax.axis_index("c")
    return lax.rem(z + sign * dz + 2 * NZ, NZ) * NY + lax.rem(y + sign * dy + 2 * NY, NY)


def place(blocks, places, normed_ref, lhs_ref, gu_ref, down_ref):
    low = lax.broadcasted_iota(jnp.int32, (512, 128), 1) < 64
    shards = []
    for block, where in zip(blocks, places):
        for k, (dz, dy) in enumerate(where):
            index = shard_index(dz % NZ, dy % NY)
            at, to = SHARD * k, 64 * len(shards)
            gu_ref[to : to + 64, :] = block[at : at + 64, :]
            for part in range(2):
                rows = pl.ds(pl.multiple_of(index * 64 + 32 * part, 32), 32)
                for j in range(5):
                    source = slice(256 * j + 128 * part, 256 * j + 128 * part + 128)
                    down_ref[rows, 128 * j : 128 * j + 128] = block[at + 64 : at + 96, source]
                down_ref[rows, 640:704] = block[at + 64 : at + 96, 1280 + 64 * part : 1344 + 64 * part]
            shards.append((dz % NZ, dy % NY))
    for j in range(0, len(shards), 2):
        halves = []
        for side in range(2):
            dz, dy = shards[j + side]
            index = shard_index(dz, dy)
            odd = lax.rem(index, 2)
            halves.append(normed_ref[odd if side == 0 else 1 - odd, lax.div(index, 2)])
        lhs_ref[:, 64 * j : 64 * j + 128] = jnp.where(low, halves[0], halves[1])


def first_kernel(places, normed_ref, *refs):
    blocks = refs[: len(places)]
    pre_ref, down_ref, lhs_ref, gu_ref = refs[len(places) :]
    place(blocks, places, normed_ref, lhs_ref, gu_ref, down_ref)
    for j in range(0, GU, 256):
        lanes = slice(j, min(j + 256, GU))
        pre_ref[:, lanes] = jnp.dot(lhs_ref[...], gu_ref[:, lanes], preferred_element_type=jnp.float32)


def down_product(hid_ref, down_ref, half, out_ref):
    x = lax.axis_index("x")
    rows = [pl.ds(pl.multiple_of(64 * lax.rem(x + (1 - 2 * half) * j + 4, 4), 64), 64) for j in range(4)]
    hid = jnp.concatenate([hid_ref[half, r, :] for r in rows], axis=0)
    for j in range(8):
        lanes = slice(256 * j, 256 * j + 256)
        out_ref[:, lanes] = lax.dot_general(
            hid, down_ref[lanes, :], (((1,), (1,)), ((), ())), preferred_element_type=jnp.float32
        ).astype(jnp.bfloat16)


def last_kernel(places, normed_ref, pre_ref, down_in_ref, *refs):
    blocks = refs[: len(places)]
    theirs_ref, hid_ref, down_ref, lhs_ref, gu_ref = refs[len(places) :]
    place(blocks, places, normed_ref, lhs_ref, gu_ref, down_ref)

    def gated(j, width):
        lanes = slice(256 * j, 256 * j + 2 * width)
        pre = pre_ref[:, lanes] + jnp.dot(lhs_ref[...], gu_ref[:, lanes], preferred_element_type=jnp.float32)
        gate, up = pre[:, :width], pre[:, width:]
        hid = (gate / (1.0 + jnp.exp(-gate)) * up).astype(jnp.bfloat16)
        hid_ref[:, :, 128 * j : 128 * j + width] = hid.reshape(2, 256, width)

    for j in range(5):
        gated(j, 128)
    gated(5, 64)
    down_product(hid_ref, down_ref, 1 - lax.axis_index("c"), theirs_ref)


def mine_kernel(hid_ref, down_ref, mine_ref):
    down_product(hid_ref, down_ref, lax.axis_index("c"), mine_ref)


def shards_of(items):
    return sum(len(where) for _, where in items)


def ffn(normed, early, late):
    down_shape = jax.ShapeDtypeStruct((D, HID), jnp.bfloat16)
    k = 64 * shards_of(early)
    pre, down = pl.pallas_call(
        functools.partial(first_kernel, [w for _, w in early]),
        out_shape=(jax.ShapeDtypeStruct((512, GU), jnp.float32), down_shape),
        in_specs=[VMEM] * (1 + len(early)),
        out_specs=(VMEM, VMEM),
        scratch_shapes=[pltpu.VMEM((512, k), jnp.bfloat16), pltpu.VMEM((k, GU), jnp.bfloat16)],
        compiler_params=pltpu.CompilerParams(vmem_limit_bytes=24 * 2**20),
        cost_estimate=pl.CostEstimate(flops=2 * 512 * k * GU, bytes_accessed=13_000_000, transcendentals=0),
        name="ffn_first",
    )(normed, *[a for a, _ in early])
    k = 64 * shards_of(late)
    half = jax.ShapeDtypeStruct((256, D), jnp.bfloat16)
    theirs, hid, down = pl.pallas_call(
        functools.partial(last_kernel, [w for _, w in late]),
        out_shape=(half, jax.ShapeDtypeStruct((2, 256, HID), jnp.bfloat16), down_shape),
        in_specs=[VMEM] * (3 + len(late)),
        out_specs=(VMEM,) * 3,
        input_output_aliases={2: 2},
        scratch_shapes=[pltpu.VMEM((512, k), jnp.bfloat16), pltpu.VMEM((k, GU), jnp.bfloat16)],
        compiler_params=pltpu.CompilerParams(vmem_limit_bytes=24 * 2**20),
        cost_estimate=pl.CostEstimate(flops=1_480_000_000, bytes_accessed=10_000_000, transcendentals=360_448),
        name="ffn_last",
    )(normed, pre, down, *[a for a, _ in late])
    mine = pl.pallas_call(
        mine_kernel,
        out_shape=half,
        in_specs=[VMEM] * 2,
        out_specs=VMEM,
        compiler_params=pltpu.CompilerParams(vmem_limit_bytes=12 * 2**20),
        cost_estimate=pl.CostEstimate(flops=740_000_000, bytes_accessed=5_000_000, transcendentals=0),
        name="ffn_mine",
    )(hid, down)
    return theirs, mine


def assemble_kernel(*refs):
    blocks, out_hbm, sems = refs[:-2], refs[-2], refs[-1]
    core, x = lax.axis_index("c"), lax.axis_index("x")
    copies = []
    for k, (block, rows) in enumerate(zip(blocks, (64, 64, 64, 64, 192, 64))):
        half = core if k < 4 else 1 - core
        sign = 1 - 2 * half
        steps = ((0,), (-1,), (2,), (1,), (0, -1, 2), (1,))[k]
        for j, step in enumerate(steps):
            row = 256 * half + 64 * lax.rem(x + sign * step + 4, 4)
            to = out_hbm.at[pl.ds(pl.multiple_of(row, 64), 64), :]
            copies.append(pltpu.make_async_copy(block.at[pl.ds(64 * j, 64), :], to, sems.at[len(copies)]))
    for copy in copies:
        copy.start()
    for copy in copies:
        copy.wait()


def assembled(blocks):
    return pl.pallas_call(
        assemble_kernel,
        out_shape=jax.ShapeDtypeStruct((512, D), jnp.bfloat16),
        in_specs=[VMEM] * len(blocks),
        out_specs=ANY,
        scratch_shapes=[pltpu.SemaphoreType.DMA((8,))],
        compiler_params=pltpu.CompilerParams(vmem_limit_bytes=6 * 2**20),
        name="assemble",
    )(*blocks)


def summed_over_x(mine, theirs):
    total = mine.astype(jnp.float32) + other_core(theirs).astype(jnp.float32)
    chunk = [total[64 * j : 64 * j + 64] for j in range(4)]
    across = hop(chunk[2].astype(jnp.bfloat16), "x", -2)
    before = hop(chunk[1].astype(jnp.bfloat16), "x", -1)
    after = hop(chunk[3].astype(jnp.bfloat16), "x", 1)
    return (chunk[0] + before + after + across).astype(jnp.bfloat16)


def copied_over_tp(rows):
    across = hop(rows, "x", -2)
    before, after = hop(rows, "x", -1), hop(rows, "x", 1)
    most = other_core(jnp.concatenate([rows, before, across], axis=0))
    return assembled([rows, before, across, after, most, other_core(after)])


def per_device(tokens, norm_gain, gate_weight, up_weight, down_weight):
    early, late = gathered(packed(gate_weight, up_weight, down_weight))
    theirs, mine = ffn(normalized(tokens, norm_gain), early, late)
    return copied_over_tp(summed_over_x(mine, theirs))


def solution(mesh):
    split = Mesh(mesh.devices.reshape(mesh.shape["rep"], 4, 8, 4, 2), ("zh", "zl", "y", "x", "c"))
    tok = P(("zh", "zl", "y"), None)
    fs, tp = ("zl", "y"), ("x", "c")
    placed = (tok, P(), P(fs, tp), P(fs, tp), P(tp, fs))
    return jax.shard_map(per_device, mesh=split, in_specs=placed, out_specs=tok, check_vma=False)
```

```python
import functools

import jax
import jax.numpy as jnp
from jax import lax
from jax.experimental import pallas as pl
from jax.experimental.pallas import tpu as pltpu
from jax.sharding import Mesh
from jax.sharding import PartitionSpec as P


NZ, NY, HID, GU = 4, 8, 704, 1408
D = 2048
SHARD = 96
VMEM = pl.BlockSpec(memory_space=pltpu.VMEM)
ANY = pl.BlockSpec(memory_space=pl.ANY)
RINGS = {"z": (("zh", "zl", "c"), 12), "y": (("y", "c"), 8), "x": (("x", "c"), 4)}


def hop(x, ring, step):
    axes, n = RINGS[ring]
    pairs = [(2 * ((i + (1 - 2 * c) * step) % n) + c, 2 * i + c) for i in range(n) for c in range(2)]
    return lax.ppermute(x, axes, pairs)


def other_core(x):
    return lax.ppermute(x, "c", [(0, 1), (1, 0)])


def pack_kernel(gate_hbm, up_hbm, down_hbm, out_ref, gate_ref, up_ref, down_ref, sems):
    pairs = ((gate_hbm, gate_ref), (up_hbm, up_ref), (down_hbm, down_ref))
    copies = [pltpu.make_async_copy(source, to, sems.at[k]) for k, (source, to) in enumerate(pairs)]
    for copy in copies:
        copy.start()
    for copy in copies:
        copy.wait()

    def pair(at, rows, a_ref, a_at, b_ref, b_at):
        for j in range(5):
            lanes = slice(128 * j, 128 * j + 128)
            out_ref[at : at + rows, 256 * j : 256 * j + 128] = a_ref[a_at : a_at + rows, lanes]
            out_ref[at : at + rows, 256 * j + 128 : 256 * j + 256] = b_ref[b_at : b_at + rows, lanes]
        last = [a_ref[a_at : a_at + rows, 640:704], b_ref[b_at : b_at + rows, 640:704]]
        out_ref[at : at + rows, 1280:1408] = jnp.concatenate(last, axis=1)

    pair(0, 64, gate_ref, 0, up_ref, 0)
    pair(64, 32, down_ref, 0, down_ref, 32)


def packed(gate, up, down):
    return pl.pallas_call(
        pack_kernel,
        out_shape=jax.ShapeDtypeStruct((SHARD, GU), jnp.bfloat16),
        in_specs=[ANY] * 3,
        out_specs=VMEM,
        scratch_shapes=[pltpu.VMEM((64, HID), jnp.bfloat16)] * 3 + [pltpu.SemaphoreType.DMA((3,))],
        compiler_params=pltpu.CompilerParams(vmem_limit_bytes=63 * 2**20),
        name="pack",
    )(gate, up, down.T)


def norm_kernel(tok_ref, gain_ref, out_ref):
    for r in range(0, 512, 64):
        tok = tok_ref[r : r + 64, :].astype(jnp.float32)
        scale = lax.rsqrt(jnp.mean(tok * tok, axis=-1, keepdims=True) + 1e-06)
        normed = tok * scale * gain_ref[...]
        for s in range(16):
            slab = normed[:, 128 * s : 128 * s + 128]
            out_ref[0, s, r : r + 64, :] = slab.astype(jnp.bfloat16)
            out_ref[1, s, r : r + 64, :] = pltpu.roll(slab, 64, 1).astype(jnp.bfloat16)


def normalized(tokens, gain):
    return pl.pallas_call(
        norm_kernel,
        out_shape=jax.ShapeDtypeStruct((2, 16, 512, 128), jnp.bfloat16),
        in_specs=[VMEM] * 2,
        out_specs=VMEM,
        compiler_params=pltpu.CompilerParams(vmem_limit_bytes=8 * 2**20),
        cost_estimate=pl.CostEstimate(flops=400_000_000, bytes_accessed=6_000_000, transcendentals=512),
        name="norm",
    )(tokens, gain.reshape(1, D))


def gathered(own):
    def whole(dz, dy):
        return [(dz, dy), (dz + 2, dy)]

    pair = jnp.concatenate([own, hop(own, "z", 2)], axis=0)
    early, late = [(pair, whole(0, 0))], []
    lo, hi = hop(pair, "y", -1), hop(pair, "y", 1)
    early.append((hop(pair, "z", -1), whole(-1, 0)))
    for k in (1, 2, 3):
        early += [(lo, whole(0, -k)), (hi, whole(0, k))]
        up, down = hop(lo, "z", -1), hop(hi, "z", 1)
        (early if k < 3 else late).extend([(up, whole(-1, -k)), (down, whole(1, k))])
        lo = hop(lo, "y", -1)
        if k < 3:
            hi = hop(hi, "y", 1)
    late += [(lo, whole(0, -4)), (hop(lo, "z", -1), whole(-1, -4))]
    return early, late


def shard_index(dz, dy):
    z, y, sign = lax.axis_index("zl"), lax.axis_index("y"), 1 - 2 * lax.axis_index("c")
    return lax.rem(z + sign * dz + 2 * NZ, NZ) * NY + lax.rem(y + sign * dy + 2 * NY, NY)


def place(blocks, places, normed_ref, lhs_ref, gu_ref, down_ref):
    low = lax.broadcasted_iota(jnp.int32, (512, 128), 1) < 64
    shards = []
    for block, where in zip(blocks, places):
        for k, (dz, dy) in enumerate(where):
            index = shard_index(dz % NZ, dy % NY)
            at, to = SHARD * k, 64 * len(shards)
            gu_ref[to : to + 64, :] = block[at : at + 64, :]
            for part in range(2):
                rows = pl.ds(pl.multiple_of(index * 64 + 32 * part, 32), 32)
                for j in range(5):
                    source = slice(256 * j + 128 * part, 256 * j + 128 * part + 128)
                    down_ref[rows, 128 * j : 128 * j + 128] = block[at + 64 : at + 96, source]
                down_ref[rows, 640:704] = block[at + 64 : at + 96, 1280 + 64 * part : 1344 + 64 * part]
            shards.append((dz % NZ, dy % NY))
    for j in range(0, len(shards), 2):
        halves = []
        for side in range(2):
            dz, dy = shards[j + side]
            index = shard_index(dz, dy)
            odd = lax.rem(index, 2)
            halves.append(normed_ref[odd if side == 0 else 1 - odd, lax.div(index, 2)])
        lhs_ref[:, 64 * j : 64 * j + 128] = jnp.where(low, halves[0], halves[1])


def first_kernel(places, normed_ref, *refs):
    blocks = refs[: len(places)]
    pre_ref, down_ref, lhs_ref, gu_ref = refs[len(places) :]
    place(blocks, places, normed_ref, lhs_ref, gu_ref, down_ref)
    for j in range(0, GU, 256):
        lanes = slice(j, min(j + 256, GU))
        pre_ref[:, lanes] = jnp.dot(lhs_ref[...], gu_ref[:, lanes], preferred_element_type=jnp.float32)


def down_product(hid_ref, down_ref, half, out_ref):
    x = lax.axis_index("x")
    rows = [pl.ds(pl.multiple_of(64 * lax.rem(x + (1 - 2 * half) * j + 4, 4), 64), 64) for j in range(4)]
    hid = jnp.concatenate([hid_ref[half, r, :] for r in rows], axis=0)
    for j in range(8):
        lanes = slice(256 * j, 256 * j + 256)
        out_ref[:, lanes] = lax.dot_general(
            hid, down_ref[lanes, :], (((1,), (1,)), ((), ())), preferred_element_type=jnp.float32
        ).astype(jnp.bfloat16)


def last_kernel(places, normed_ref, pre_ref, down_in_ref, *refs):
    blocks = refs[: len(places)]
    theirs_ref, hid_ref, down_ref, lhs_ref, gu_ref = refs[len(places) :]
    place(blocks, places, normed_ref, lhs_ref, gu_ref, down_ref)

    def gated(j, width):
        lanes = slice(256 * j, 256 * j + 2 * width)
        pre = pre_ref[:, lanes] + jnp.dot(lhs_ref[...], gu_ref[:, lanes], preferred_element_type=jnp.float32)
        gate, up = pre[:, :width], pre[:, width:]
        hid = (gate / (1.0 + jnp.exp(-gate)) * up).astype(jnp.bfloat16)
        hid_ref[:, :, 128 * j : 128 * j + width] = hid.reshape(2, 256, width)

    for j in range(5):
        gated(j, 128)
    gated(5, 64)
    down_product(hid_ref, down_ref, 1 - lax.axis_index("c"), theirs_ref)


def mine_kernel(hid_ref, down_ref, mine_ref):
    down_product(hid_ref, down_ref, lax.axis_index("c"), mine_ref)


def shards_of(items):
    return sum(len(where) for _, where in items)


def ffn(normed, early, late):
    down_shape = jax.ShapeDtypeStruct((D, HID), jnp.bfloat16)
    k = 64 * shards_of(early)
    pre, down = pl.pallas_call(
        functools.partial(first_kernel, [w for _, w in early]),
        out_shape=(jax.ShapeDtypeStruct((512, GU), jnp.float32), down_shape),
        in_specs=[VMEM] * (1 + len(early)),
        out_specs=(VMEM, VMEM),
        scratch_shapes=[pltpu.VMEM((512, k), jnp.bfloat16), pltpu.VMEM((k, GU), jnp.bfloat16)],
        compiler_params=pltpu.CompilerParams(vmem_limit_bytes=24 * 2**20),
        cost_estimate=pl.CostEstimate(flops=2 * 512 * k * GU, bytes_accessed=13_000_000, transcendentals=0),
        name="ffn_first",
    )(normed, *[a for a, _ in early])
    k = 64 * shards_of(late)
    half = jax.ShapeDtypeStruct((256, D), jnp.bfloat16)
    theirs, hid, down = pl.pallas_call(
        functools.partial(last_kernel, [w for _, w in late]),
        out_shape=(half, jax.ShapeDtypeStruct((2, 256, HID), jnp.bfloat16), down_shape),
        in_specs=[VMEM] * (3 + len(late)),
        out_specs=(VMEM,) * 3,
        input_output_aliases={2: 2},
        scratch_shapes=[pltpu.VMEM((512, k), jnp.bfloat16), pltpu.VMEM((k, GU), jnp.bfloat16)],
        compiler_params=pltpu.CompilerParams(vmem_limit_bytes=24 * 2**20),
        cost_estimate=pl.CostEstimate(flops=1_480_000_000, bytes_accessed=10_000_000, transcendentals=360_448),
        name="ffn_last",
    )(normed, pre, down, *[a for a, _ in late])
    mine = pl.pallas_call(
        mine_kernel,
        out_shape=half,
        in_specs=[VMEM] * 2,
        out_specs=VMEM,
        compiler_params=pltpu.CompilerParams(vmem_limit_bytes=12 * 2**20),
        cost_estimate=pl.CostEstimate(flops=740_000_000, bytes_accessed=5_000_000, transcendentals=0),
        name="ffn_mine",
    )(hid, down)
    return theirs, mine


def assemble_kernel(*refs):
    blocks, out_hbm, sems = refs[:-2], refs[-2], refs[-1]
    core, x = lax.axis_index("c"), lax.axis_index("x")
    copies = []
    for k, (block, rows) in enumerate(zip(blocks, (64, 64, 64, 64, 256))):
        half = core if k < 4 else 1 - core
        sign = 1 - 2 * half
        steps = ((0,), (-1,), (2,), (1,), (0, -1, 2, 1))[k]
        for j, step in enumerate(steps):
            row = 256 * half + 64 * lax.rem(x + sign * step + 4, 4)
            to = out_hbm.at[pl.ds(pl.multiple_of(row, 64), 64), :]
            copies.append(pltpu.make_async_copy(block.at[pl.ds(64 * j, 64), :], to, sems.at[len(copies)]))
    for copy in copies:
        copy.start()
    for copy in copies:
        copy.wait()


def assembled(blocks):
    return pl.pallas_call(
        assemble_kernel,
        out_shape=jax.ShapeDtypeStruct((512, D), jnp.bfloat16),
        in_specs=[VMEM] * len(blocks),
        out_specs=ANY,
        scratch_shapes=[pltpu.SemaphoreType.DMA((8,))],
        compiler_params=pltpu.CompilerParams(vmem_limit_bytes=6 * 2**20),
        name="assemble",
    )(*blocks)


def summed_over_x(mine, theirs):
    total = mine.astype(jnp.float32) + other_core(theirs).astype(jnp.float32)
    chunk = [total[64 * j : 64 * j + 64] for j in range(4)]
    across = hop(chunk[2].astype(jnp.bfloat16), "x", -2)
    before = hop(chunk[1].astype(jnp.bfloat16), "x", -1)
    after = hop(chunk[3].astype(jnp.bfloat16), "x", 1)
    return (chunk[0] + before + after + across).astype(jnp.bfloat16)


def copied_over_tp(rows):
    across = hop(rows, "x", -2)
    before, after = hop(rows, "x", -1), hop(rows, "x", 1)
    both = jnp.concatenate([rows, before, across, after], axis=0)
    return assembled([rows, before, across, after, other_core(both)])


def per_device(tokens, norm_gain, gate_weight, up_weight, down_weight):
    early, late = gathered(packed(gate_weight, up_weight, down_weight))
    theirs, mine = ffn(normalized(tokens, norm_gain), early, late)
    return copied_over_tp(summed_over_x(mine, theirs))


def solution(mesh):
    split = Mesh(mesh.devices.reshape(mesh.shape["rep"], 4, 8, 4, 2), ("zh", "zl", "y", "x", "c"))
    tok = P(("zh", "zl", "y"), None)
    fs, tp = ("zl", "y"), ("x", "c")
    placed = (tok, P(), P(fs, tp), P(fs, tp), P(tp, fs))
    return jax.shard_map(per_device, mesh=split, in_specs=placed, out_specs=tok, check_vma=False)
```
